32 devices in a mesh: dp: 4 (over y, x), kv: 4 (over z), tp: 2 (over core).
Axes of the slice: x: 2, y: 2, z: 4, core: 2. Of those that a mesh axis runs over, the one named last changes fastest.
Arguments:
- tokens: bfloat16 [2048, 2048], P('dp', 'kv'), may hold values from -70 to 70
- pre_gain: float32 [2048], replicated, may hold values from 0.1 to 1.9
- query_weight: bfloat16 [2048, 1024], P(None, 'tp'), may hold values from -0.125 to 0.125
- key_weight: bfloat16 [2048, 1024], P(None, 'tp'), may hold values from -0.125 to 0.125
- value_weight: bfloat16 [2048, 1024], P(None, 'tp'), may hold values from -0.125 to 0.125
- gate_weight: bfloat16 [2048, 1024], P(None, 'tp'), may hold values from -0.125 to 0.125
- beta_weight: bfloat16 [2048, 8], replicated, may hold values from -0.125 to 0.125
- decay_weight: bfloat16 [2048, 8], replicated, may hold values from -0.125 to 0.125
- decay_log: float32 [8], P('tp'), may hold values from -3 to 0.5
- head_gain: float32 [128], replicated, may hold values from 0.1 to 1.9
- out_weight: bfloat16 [1024, 2048], P('tp', 'kv'), may hold values from -1 to 1
- post_gain: float32 [2048], P(('kv', 'tp')), may hold values from 0.1 to 1.9
- saved_state: float32 [512, 8, 128, 128], P(('dp', 'kv'), 'tp'), may hold values from -4 to 4
- earlier_keys: bfloat16 [512, 4, 8, 128], P(('dp', 'kv'), None, 'tp'), may hold values from -6 to 6
- earlier_values: bfloat16 [512, 4, 8, 128], P(('dp', 'kv'), None, 'tp'), may hold values from -6 to 6
- earlier_rates: float32 [512, 4, 8], P(('dp', 'kv'), None, 'tp'), may hold values from 0.05 to 0.95
- earlier_decays: float32 [512, 4, 8], P(('dp', 'kv'), None, 'tp'), may hold values from -1.5 to -0.02
- accepted: int32 [512], P(('dp', 'kv')), may hold values from 0 to 4
Outputs:
- mixed: bfloat16 [2048, 2048], P('dp', ('kv', 'tp'))
- committed: float32 [512, 8, 128, 128], P(('dp', 'kv'), 'tp')
The draws below stay inside these ranges and needn't reach their ends.
All inputs are finite; a program needn't handle non-finite values.
Results may differ from the reference program's by a relative error of at most 0.011.
Values may be sent and summed in bfloat16 or wider, within the bound.
A program may use at most 128 MiB of HBM per device.

```python
import jax
import jax.numpy as jnp
from jax import lax

D = 2048
HEADS = 8
HEAD = 128
PROPOSALS = 4
SEQS = 512
ROWS = 2048


def draw_tokens(key, part):
    columns = jnp.arange(D, dtype=jnp.float32)
    rising = 1.0 + 3.0 * columns / D
    base = jnp.clip(jax.random.normal(key, (ROWS, D), jnp.float32), -5.0, 5.0)
    return (base * rising).astype(jnp.bfloat16)


def draw_out_weight(key, part):
    columns = jnp.arange(D, dtype=jnp.float32)
    rising = (1.0 + 3.0 * columns / D) * (HEADS * HEAD) ** (-0.5)
    base = jnp.clip(jax.random.normal(key, (HEADS * HEAD, D), jnp.float32), -6.0, 6.0)
    return jnp.clip(base * rising, -1.0, 1.0).astype(jnp.bfloat16)


def place_ends(entries, stream_key, smallest, top_value):
    dims = entries.shape
    spot = [jax.random.randint(jax.random.fold_in(stream_key, axis), (), 0, dims[axis]) for axis in range(len(dims))]
    entries = entries.at[tuple(spot)].set(smallest)
    longest = dims.index(max(dims))
    spot[longest] = (spot[longest] + 1) % dims[longest]
    return entries.at[tuple(spot)].set(top_value)


def level_of(key, extent, cuts, least, high):
    def one(dim, shards_of):
        heights = jax.random.uniform(jax.random.fold_in(jax.random.fold_in(key, 6), dim), (shards_of,), jnp.float32, least / len(cuts), high / len(cuts))
        return jnp.repeat(jnp.exp(heights), extent[dim] // shards_of).reshape((-1,) + (1,) * (len(extent) - dim - 1))

    loudness = one(*cuts[0])
    for cut in cuts[1:]:
        loudness = loudness * one(*cut)
    return loudness


def normal_values(rng, extent, deviation, most, cuts=(), kind=jnp.bfloat16):
    values = deviation * jax.random.normal(rng, extent, jnp.float32)
    if cuts:
        values = values * level_of(rng, extent, cuts, -0.22, 0.18)
    return jnp.clip(values, -most, most).astype(kind)


def setup_inputs(seed: int = 0) -> dict:
    splits = jax.random.split(jax.random.key(seed), 19)
    return {
        "tokens": draw_tokens(jax.random.fold_in(splits[18], 71), 0),
        "pre_gain": jnp.clip(1.0 + 0.18 * jax.random.normal(splits[1], (D,), jnp.float32), 0.1, 1.9),
        "query_weight": normal_values(splits[2], (D, HEADS * HEAD), D ** -0.5, 0.125, ((1, 2),)),
        "key_weight": normal_values(splits[3], (D, HEADS * HEAD), D ** -0.5, 0.125, ((1, 2),)),
        "value_weight": normal_values(splits[4], (D, HEADS * HEAD), D ** -0.5, 0.125, ((1, 2),)),
        "gate_weight": normal_values(splits[5], (D, HEADS * HEAD), D ** -0.5, 0.125, ((1, 2),)),
        "beta_weight": normal_values(splits[6], (D, HEADS), D ** -0.5, 0.125),
        "decay_weight": normal_values(splits[7], (D, HEADS), D ** -0.5, 0.125),
        "decay_log": jnp.clip(-3.0 + 3.5 * jax.random.uniform(splits[8], (HEADS,), jnp.float32) ** level_of(splits[8], (HEADS,), ((0, 2),), -0.2, 0.2), -3.0, 0.5),
        "head_gain": jnp.clip(1.0 + 0.18 * jax.random.normal(splits[9], (HEAD,), jnp.float32), 0.1, 1.9),
        "out_weight": draw_out_weight(jax.random.fold_in(splits[18], 71), 0),
        "post_gain": jnp.clip(1.0 + 0.18 * jax.random.normal(splits[11], (D,), jnp.float32), 0.1, 1.9),
        "saved_state": normal_values(splits[12], (SEQS, HEADS, HEAD, HEAD), 0.3, 4.0, ((0, 16), (1, 2)), jnp.float32),
        "earlier_keys": normal_values(splits[13], (SEQS, PROPOSALS, HEADS, HEAD), 1.0, 6.0, ((0, 16), (2, 2))),
        "earlier_values": normal_values(splits[14], (SEQS, PROPOSALS, HEADS, HEAD), 1.0, 6.0, ((0, 16), (2, 2))),
        "earlier_rates": jnp.clip(0.05 + 0.9 * jax.random.uniform(splits[15], (SEQS, PROPOSALS, HEADS), jnp.float32) ** level_of(splits[15], (SEQS, PROPOSALS, HEADS), ((0, 16), (2, 2)), -0.2, 0.2), 0.05, 0.95),
        "earlier_decays": jnp.clip(-1.5 + 1.48 * jax.random.uniform(splits[16], (SEQS, PROPOSALS, HEADS), jnp.float32) ** level_of(splits[16], (SEQS, PROPOSALS, HEADS), ((0, 16), (2, 2)), -0.2, 0.2), -1.5, -0.02),
        "accepted": place_ends(jax.random.randint(splits[17], (SEQS,), 0, PROPOSALS + 1), jax.random.fold_in(splits[17], 1), 0, PROPOSALS).astype(jnp.int32),
    }


def unit_norm(values):
    return values * lax.rsqrt(lax.optimization_barrier(jnp.sum(values * values, axis=-1, keepdims=True)) + 1e-06)

def advance(current, key_row, value_row, rate_now, log_decay):
    recalled = lax.optimization_barrier(jnp.sum(key_row[..., :, None] * current, axis=-2))
    rate_cube = rate_now[..., None, None]
    current = current - rate_cube * key_row[..., :, None] * recalled[..., None, :]
    return jnp.exp(log_decay)[..., None, None] * current + rate_cube * key_row[..., :, None] * value_row[..., None, :]

def run_heads(saved_state, earlier_keys, earlier_values, earlier_rates, earlier_decays, accepted, queries, keys_unit, values_act, rates, decays):
    current = saved_state
    proposals = earlier_keys.shape[1]
    for position in range(proposals):
        live = (position < accepted).astype(jnp.float32)
        live = live.reshape(live.shape + (1,) * (earlier_rates.ndim - 2))
        current = advance(current, earlier_keys[:, position], earlier_values[:, position], earlier_rates[:, position] * live, earlier_decays[:, position] * live)
    committed = current
    outputs = []
    for position in range(proposals):
        current = advance(current, keys_unit[:, position], values_act[:, position], rates[:, position], decays[:, position])
        outputs.append(lax.optimization_barrier(jnp.sum(queries[:, position][..., :, None] * current, axis=-2)))
    return (committed, jnp.stack(outputs, axis=1))

def reference(tokens, pre_gain, query_weight, key_weight, value_weight, gate_weight, beta_weight, decay_weight, decay_log, head_gain, out_weight, post_gain, saved_state, earlier_keys, earlier_values, earlier_rates, earlier_decays, accepted):
    widened = tokens.astype(jnp.float32)
    inverse = lax.rsqrt(lax.optimization_barrier(jnp.mean(widened * widened, axis=1, keepdims=True)) + 1e-06)
    scaled = (widened * pre_gain).astype(jnp.bfloat16)

    def project(weight):
        return jnp.dot(scaled, weight, preferred_element_type=jnp.float32) * inverse

    def heads_of(values):
        return values.reshape(SEQS, PROPOSALS, HEADS, HEAD)
    queries = unit_norm(jax.nn.silu(heads_of(project(query_weight)))) * HEAD ** (-0.5)
    keys_unit = unit_norm(jax.nn.silu(heads_of(project(key_weight))))
    values_act = jax.nn.silu(heads_of(project(value_weight)))
    gates_raw = heads_of(project(gate_weight))
    rates = jax.nn.sigmoid(project(beta_weight)).reshape(SEQS, PROPOSALS, HEADS)
    decays = -jnp.exp(decay_log) * jax.nn.softplus(project(decay_weight)).reshape(SEQS, PROPOSALS, HEADS)
    earlier_unit = unit_norm(earlier_keys.astype(jnp.float32))
    earlier_vals = earlier_values.astype(jnp.float32)

    def per_head(items):
        return run_heads(items[0], items[1], items[2], items[3], items[4], accepted, items[5], items[6], items[7], items[8], items[9])
    items = (jnp.moveaxis(saved_state, 1, 0), jnp.moveaxis(earlier_unit, 2, 0), jnp.moveaxis(earlier_vals, 2, 0), jnp.moveaxis(earlier_rates, 2, 0), jnp.moveaxis(earlier_decays, 2, 0), jnp.moveaxis(queries, 2, 0), jnp.moveaxis(keys_unit, 2, 0), jnp.moveaxis(values_act, 2, 0), jnp.moveaxis(rates, 2, 0), jnp.moveaxis(decays, 2, 0))
    committed, reads = lax.map(per_head, items)
    committed = jnp.moveaxis(committed, 0, 1)
    reads = jnp.moveaxis(reads, 0, 2)
    normed = reads * lax.rsqrt(lax.optimization_barrier(jnp.mean(reads * reads, axis=-1, keepdims=True)) + 1e-06) * head_gain
    attended = (normed * jax.nn.silu(gates_raw)).reshape(ROWS, HEADS * HEAD).astype(jnp.bfloat16)
    projected = jnp.dot(attended, out_weight, preferred_element_type=jnp.float32)
    factor = lax.rsqrt(lax.optimization_barrier(jnp.mean(projected * projected, axis=1, keepdims=True)) + 1e-06)
    mixed = (projected * factor * post_gain).astype(jnp.bfloat16)
    return (mixed, committed)
```

```python
import functools

import jax
import jax.numpy as jnp
from jax import lax
from jax.experimental import pallas as pl
from jax.experimental.pallas import tpu as pltpu
from jax.sharding import PartitionSpec as P

F32 = jnp.float32
BF16 = jnp.bfloat16
EPS = 1e-06
MESH_IDS = pl.DeviceIdType.MESH
VMEM_BYTES = 36 * 1024 * 1024


def mm(a, b):
    return jnp.dot(a, b, preferred_element_type=F32)


def mm_nt(a, b):
    return lax.dot_general(a, b, (((1,), (1,)), ((), ())), preferred_element_type=F32)


def mm_tn(a, b):
    return lax.dot_general(a, b, (((0,), (0,)), ((), ())), preferred_element_type=F32)


def mm_exact(a, b):
    return jnp.dot(a, b, preferred_element_type=F32, precision=lax.Precision.HIGHEST)


def unit(values):
    return values * lax.rsqrt(jnp.sum(values * values, axis=-1, keepdims=True) + EPS)


def silu(values):
    return values / (1.0 + jnp.exp(-values))


def masks_of(rows, proposals):
    r = lax.broadcasted_iota(jnp.int32, (rows, rows), 0)
    c = lax.broadcasted_iota(jnp.int32, (rows, rows), 1)
    same = (r // proposals) == (c // proposals)
    return same, same & (c <= r), same & (c < r)


def per_sequence(operands, state_of, proposals, rows):
    size = operands[0].shape[1]
    group = 16
    seqs = group // proposals
    stack = group * len(operands)
    row = lax.broadcasted_iota(jnp.int32, (stack, size), 0)
    owner = (row % group) // proposals
    outs = [[] for _ in operands]
    for g in range(rows // group):
        x = jnp.concatenate([o[g * group:(g + 1) * group] for o in operands], axis=0)
        lhs = jnp.concatenate(
            [jnp.where(owner == s, x, 0.0).astype(BF16) for s in range(seqs)], axis=1
        )
        rhs = state_of(g * seqs, seqs).reshape(seqs * size, size).astype(BF16)
        y = mm(lhs, rhs)
        for i in range(len(operands)):
            outs[i].append(y[i * group:(i + 1) * group])
    return [jnp.concatenate(o, axis=0) for o in outs]


def solve(keys, values, recalled, rate, decay_pairs, gamma, strict):
    kb = keys.astype(BF16)
    low = (jnp.where(strict, decay_pairs * mm_nt(kb, kb), 0.0) * rate).astype(BF16)
    rhs = rate * (values - gamma * recalled)
    square = mm(low, low).astype(BF16)
    x = rhs + mm(square, rhs.astype(BF16))
    return x - mm(low, x.astype(BF16))


def head_masks(rows, group, heads):
    r = lax.broadcasted_iota(jnp.int32, (rows, rows), 0)
    c = lax.broadcasted_iota(jnp.int32, (rows, rows), 1)
    same = ((r // group) == (c // group)) & ((r % heads) == (c % heads))
    return same & (c <= r), same & (c < r)


def commit_table(proposals, heads, rates, decays, accepted):
    seqs = accepted.shape[1]
    live = [accepted > p for p in range(proposals)]
    rate = jnp.concatenate([jnp.where(live[p], rates[p], 0.0) for p in range(proposals)], axis=0)
    sums = [jnp.where(live[0], decays[0], 0.0)]
    for p in range(1, proposals):
        sums.append(sums[-1] + jnp.where(live[p], decays[p], 0.0))
    cum = jnp.concatenate(sums, axis=0)
    last = jnp.concatenate([sums[-1]] * proposals, axis=0)
    used = 3 * proposals * heads
    table = jnp.concatenate([rate, cum, last], axis=0)
    table = jnp.concatenate([table, jnp.zeros((used, 128 - seqs), F32)], axis=1)
    table = jnp.concatenate([table, jnp.zeros((128 - used, 128), F32)], axis=0)
    return table.T


def commit_block(block, proposals, heads, table, keys_raw, values, masks, com, sbf):
    rows, size = keys_raw.shape
    group = proposals * heads
    seqs = rows // group
    incl, strict = masks
    spread = jnp.concatenate(
        [
            jnp.broadcast_to(table[block * seqs + i:block * seqs + i + 1, :], (group, 128))
            for i in range(seqs)
        ],
        axis=0,
    )
    lane = lax.broadcasted_iota(jnp.int32, (rows, 128), 1)
    slot = lax.broadcasted_iota(jnp.int32, (rows, 128), 0) % group

    def column(k):
        return jnp.sum(jnp.where(lane == k * group + slot, spread, 0.0), axis=1, keepdims=True)

    rate, g_col, g_last = column(0), column(1), column(2)
    g_row = jnp.broadcast_to(g_col, (rows, rows)).T
    pairs = jnp.exp(jnp.where(incl, g_col - g_row, -1e30))
    keys = unit(keys_raw.astype(F32))
    owner = lax.broadcasted_iota(jnp.int32, (group, size), 0) % heads

    def widen(x):
        return jnp.concatenate(
            [jnp.where(owner == h, x, 0.0).astype(BF16) for h in range(heads)], axis=1
        )

    recalled = jnp.concatenate(
        [
            mm(
                widen(keys[i * group:(i + 1) * group]),
                com[block * seqs + i].reshape(heads * size, size).astype(BF16),
            )
            for i in range(seqs)
        ],
        axis=0,
    )
    w = solve(keys, values.astype(F32), recalled, rate, pairs, jnp.exp(g_col), strict)
    scaled_keys = (keys * jnp.exp(g_last - g_col)).astype(BF16)
    whole = jnp.broadcast_to(jnp.exp(g_last), (rows, size))
    for i in range(seqs):
        seq = block * seqs + i
        span = slice(i * group, (i + 1) * group)
        add = mm_tn(scaled_keys[span], widen(w[span]))
        for h in range(heads):
            keep = whole[i * group + h:i * group + h + 1]
            new = keep * com[seq, h] + add[:, h * size:(h + 1) * size]
            com[seq, h] = new
            sbf[h, seq] = new.astype(BF16)


def layer_kernel(
    kv, tp, proposals, heads, model_width,
    tokens, gains_h, qw, kw, vw, gw, beta_h, decay_h, log_h, head_gain_h, ow, post_h, state,
    ekeys_h, evalues_h, erates_h, edecays_h, accepted_h,
    out, com,
    tokv, tok, wv, sbf, owv, acc, sacc, att, passed, part, give, take, sums, sumall,
    gains, beta_t, decay_t, log_rate, head_gain, post, ekeys, evalues, erates, edecays, accepted,
    w_sem, s_sem, ow_sem, own_sem, small_sem, tok_send, tok_recv, half_send, half_recv,
    att_send, att_recv, tp_send, tp_recv, sum_send, sum_recv,
):
    me = lax.axis_index("kv")
    core = lax.axis_index("tp")
    rows, chunk = tok.shape[1], tok.shape[2]
    size = head_gain.shape[1]
    cols = out.shape[1]
    weights = (qw, kw, vw, gw)

    def source(d):
        return lax.rem(me - d + kv, kv)

    def target(d):
        return lax.rem(me + d, kv)

    barrier = pltpu.get_barrier_semaphore()
    group = kv * tp
    flat = me * tp + core

    def peer(o):
        other = lax.rem(flat + o, group)
        return {"kv": other // tp, "tp": lax.rem(other, tp)}

    for o in range(1, group):
        pl.semaphore_signal(barrier, inc=1, device_id=peer(o), device_id_type=MESH_IDS)

    local = {}
    local["tok"] = pltpu.make_async_copy(tokens, tokv, own_sem)
    local["tok"].start()
    pairs_small = (
        (ekeys_h, ekeys), (evalues_h, evalues), (erates_h, erates), (edecays_h, edecays),
        (accepted_h, accepted), (gains_h, gains), (beta_h, beta_t), (decay_h, decay_t),
        (log_h, log_rate), (head_gain_h, head_gain), (post_h, post),
    )
    for i, (src, dst) in enumerate(pairs_small):
        local["small", i] = pltpu.make_async_copy(src, dst, small_sem.at[i])
        local["small", i].start()
    block_rows = min(128, ekeys.shape[0])
    blocks_n = ekeys.shape[0] // block_rows
    block_seqs = state.shape[0] // blocks_n
    for b in range(blocks_n):
        span = pl.ds(b * block_seqs, block_seqs)
        local["s", b] = pltpu.make_async_copy(state.at[span], com.at[span], s_sem.at[b])
        local["s", b].start()
    for d in range(kv):
        for i in range(4):
            local["w", i, d] = pltpu.make_async_copy(
                weights[i].at[pl.ds(source(d) * chunk, chunk), :], wv.at[i, d], w_sem.at[i, d]
            )
            local["w", i, d].start()
    for o in range(tp):
        half = lax.rem(core + o, tp)
        if len(ow.shape) == 3:
            src = ow.at[half]
        else:
            src = ow.at[:, pl.ds(pl.multiple_of(half * cols, 128), cols)]
        local["o", o] = pltpu.make_async_copy(src, owv.at[o], ow_sem.at[o])
        local["o", o].start()

    local["tok"].wait()
    pl.semaphore_wait(barrier, group - 1)

    part_rows = rows // tp
    mine_rows = pl.ds(pl.multiple_of(core * part_rows, part_rows), part_rows)
    sent = {}
    halves = {}
    for d in range(1, kv):
        sent[d] = pltpu.make_async_remote_copy(
            src_ref=tokv.at[
                pl.ds(pl.multiple_of(target(d) * rows + core * part_rows, part_rows), part_rows), :
            ],
            dst_ref=tok.at[d, mine_rows],
            send_sem=tok_send.at[d],
            recv_sem=tok_recv.at[d],
            device_id={"kv": target(d)},
            device_id_type=MESH_IDS,
        )
        sent[d].start()

    def hand_over(d):
        sent[d].wait_recv()
        for o in range(1, tp):
            halves[d, o] = pltpu.make_async_remote_copy(
                src_ref=tok.at[d, mine_rows],
                dst_ref=tok.at[d, mine_rows],
                send_sem=half_send.at[d, o],
                recv_sem=half_recv.at[d, o],
                device_id={"tp": lax.rem(core + o, tp)},
                device_id_type=MESH_IDS,
            )
            halves[d, o].start()

    def project(d, squares):
        if d > 0:
            for o in range(1, tp):
                halves[d, o].wait_recv()
        c = source(d)
        span = pl.ds(pl.multiple_of(c * chunk, 128), chunk)
        if d == 0:
            wide = tokv[pl.ds(pl.multiple_of(me * rows, rows), rows), :].astype(F32)
        else:
            wide = tok[d].astype(F32)
        scaled = (wide * gains[:, span]).astype(BF16)
        thin = mm_nt(scaled, jnp.concatenate([beta_t[:, span], decay_t[:, span]], axis=0))
        if d == 0:
            sacc[...] = thin
        else:
            sacc[...] += thin
        for i in range(4):
            local["w", i, d].wait()
            y = mm(scaled, wv[i, d])
            if d == 0:
                acc[i] = y
            else:
                acc[i] += y
        return squares + jnp.sum(wide * wide, axis=1, keepdims=True)

    for i in range(len(pairs_small)):
        local["small", i].wait()
    table = commit_table(proposals, heads, erates[...], edecays[...], accepted[...])
    commit_masks = head_masks(block_rows, proposals * heads, heads)
    squares = jnp.zeros((rows, 1), F32)
    steps = max(blocks_n, kv)
    for b in range(steps):
        if b < blocks_n:
            span = slice(b * block_rows, (b + 1) * block_rows)
            local["s", b].wait()
            commit_block(
                b, proposals, heads, table, ekeys[span], evalues[span], commit_masks, com, sbf
            )
        if 1 <= b < kv:
            hand_over(b)
        if b >= 1 and b - 1 < kv - 1:
            squares = project(b - 1, squares)
    squares = project(kv - 1, squares)
    inverse = lax.rsqrt(squares / model_width + EPS)

    same, incl, strict = masks_of(rows, proposals)
    all_heads = heads * tp
    pad = jnp.zeros((rows, 128 - 2 * all_heads), F32)
    raw = jnp.concatenate([sacc[...] * inverse, pad], axis=1)
    raw = pltpu.roll(raw, lax.rem(128 - core * heads, 128), axis=1)
    rates = 1.0 / (1.0 + jnp.exp(-raw))
    soft = jnp.maximum(raw, 0.0) + jnp.log1p(jnp.exp(-jnp.abs(raw)))
    speed = jnp.concatenate(
        [
            jnp.zeros((1, all_heads), F32), jnp.exp(log_rate[...]),
            jnp.zeros((1, 128 - all_heads - heads), F32),
        ],
        axis=1,
    )
    cum = -speed * soft
    place = lax.broadcasted_iota(jnp.int32, (rows, 128), 0) % proposals
    step = 1
    while step < proposals:
        cum = cum + jnp.where(place >= step, pltpu.roll(cum, step, axis=0), 0.0)
        step *= 2
    cum_t = cum.T

    def hop(way, s, h):
        step = 1 if way == 0 else kv - 1
        return pltpu.make_async_remote_copy(
            src_ref=att.at[h] if s == 0 else passed.at[way, s, h],
            dst_ref=passed.at[way, s + 1, h],
            send_sem=att_send.at[way, s, h],
            recv_sem=att_recv.at[way, s + 1, h],
            device_id={"kv": lax.rem(me + step, kv)},
            device_id_type=MESH_IDS,
        )

    def arrives(way, s):
        return me - s >= 0 if way == 0 else me + s < kv

    def leaves(way):
        return me + 1 < kv if way == 0 else me >= 1

    def advance(turn):
        for s in range(kv):
            h = turn - s
            if not 0 <= h < heads:
                continue
            for way in range(2):
                if s == 0:
                    @pl.when(leaves(way))
                    def _():
                        hop(way, 0, h).start()
                else:
                    @pl.when(arrives(way, s))
                    def _():
                        hop(way, s - 1, h).wait_recv()
                    if s < kv - 1:
                        @pl.when(arrives(way, s) & leaves(way))
                        def _():
                            hop(way, s, h).start()

    def settle():
        for s in range(kv - 1):
            for way in range(2):
                @pl.when(arrives(way, s) & leaves(way))
                def _():
                    for h in range(heads):
                        hop(way, s, h).wait_send()

    for first in range(heads):
        batch = range(first, first + 1)
        query, key, pairs, gamma, w, asked, reads = {}, {}, {}, {}, {}, {}, {}
        recalled = {}
        for h in batch:
            block = slice(h * size, (h + 1) * size)
            query[h] = unit(silu(acc[0, :, block] * inverse)) * size ** (-0.5)
            key[h] = unit(silu(acc[1, :, block] * inverse))
            pairs[h] = jnp.exp(jnp.where(incl, cum[:, all_heads + h:all_heads + h + 1] - cum_t[all_heads + h:all_heads + h + 1, :], -1e30))
            gamma[h] = jnp.exp(cum[:, all_heads + h:all_heads + h + 1])
        for h in batch:
            recalled[h], asked[h] = per_sequence(
                [key[h], query[h]], lambda s, n, h=h: sbf[h, s:s + n], proposals, rows
            )
        for h in batch:
            value = silu(acc[2, :, h * size:(h + 1) * size] * inverse)
            w[h] = solve(key[h], value, recalled[h], rates[:, h:h + 1], pairs[h], gamma[h], strict)
        for h in batch:
            mix = (pairs[h] * mm_nt(query[h].astype(BF16), key[h].astype(BF16))).astype(BF16)
            reads[h] = gamma[h] * asked[h] + mm(mix, w[h].astype(BF16))
        for h in batch:
            gate = silu(acc[3, :, h * size:(h + 1) * size] * inverse)
            scale = lax.rsqrt(jnp.mean(reads[h] * reads[h], axis=-1, keepdims=True) + EPS)
            att[h] = (reads[h] * scale * head_gain[...] * gate).astype(BF16)
        for h in batch:
            advance(h)

    for o in range(tp):
        local["o", o].wait()

    def swap(c, o):
        return pltpu.make_async_remote_copy(
            src_ref=give.at[c, o],
            dst_ref=take.at[c, o],
            send_sem=tp_send.at[c, o],
            recv_sem=tp_recv.at[c, o],
            device_id={"tp": lax.rem(core + o, tp)},
            device_id_type=MESH_IDS,
        )

    def combine(c, pieces):
        rows_in = jnp.concatenate(pieces, axis=1)
        for o in range(1, tp):
            give[c, o] = mm(rows_in, owv[o]).astype(BF16)
            swap(c, o).start()
        part[c] = mm(rows_in, owv[0])

    def finish(c):
        own = part[c]
        for o in range(1, tp):
            swap(c, o).wait_recv()
            own = own + take[c, o].astype(F32)
        part[c] = own
        total = jnp.sum(own * own, axis=1, keepdims=True)
        sums[pl.ds(c, 1), :] = jnp.broadcast_to(total, (rows, rows)).T[0:1]

    def blocks(turn):
        if turn < heads:
            return [(True, me, None)]
        s = turn - heads + 1
        return [(arrives(way, s), me - s if way == 0 else me + s, way) for way in range(2)]

    combine(me, [att[h] for h in range(heads)])
    for turn in range(heads, heads + kv - 1):
        advance(turn)
        s = turn - heads + 1
        for here, c, way in blocks(turn):
            @pl.when(here)
            def _():
                combine(c, [passed[way, s, h] for h in range(heads)])
        if s == 1:
            finish(me)
        else:
            for here, c, way in blocks(turn - 1):
                @pl.when(here)
                def _():
                    finish(c)
    if kv > 1:
        for here, c, way in blocks(heads + kv - 2):
            @pl.when(here)
            def _():
                finish(c)
    else:
        finish(me)
    tells = {}
    for o in range(1, group):
        tells[o] = pltpu.make_async_remote_copy(
            src_ref=sums,
            dst_ref=sumall.at[o],
            send_sem=sum_send.at[o],
            recv_sem=sum_recv.at[o],
            device_id=peer(o),
            device_id_type=MESH_IDS,
        )
        tells[o].start()
    settle()
    for d in range(1, kv):
        sent[d].wait_send()
        for o in range(1, tp):
            halves[d, o].wait_send()
    for c in range(kv):
        for o in range(1, tp):
            swap(c, o).wait_send()
    totals = sums[...]
    for o in range(1, group):
        tells[o].wait_recv()
        totals = totals + sumall[o]
    sums_factor = lax.rsqrt(totals / model_width + EPS)
    for o in range(1, group):
        tells[o].wait_send()
    for c in range(kv):
        factor = jnp.broadcast_to(sums_factor[c:c + 1, :], (rows, rows)).T[:, 0:1]
        out[c * rows:(c + 1) * rows, :] = (part[c] * factor * post[...]).astype(BF16)


def make_local(mesh):
    kv = mesh.shape["kv"]
    tp = mesh.shape["tp"]

    def local(
        tokens, pre_gain, query_weight, key_weight, value_weight, gate_weight, beta_weight,
        decay_weight, decay_log, head_gain, out_weight, post_gain, saved_state, earlier_keys,
        earlier_values, earlier_rates, earlier_decays, accepted,
    ):
        seqs, heads, size = saved_state.shape[:3]
        proposals = earlier_keys.shape[1]
        rows = seqs * proposals
        width = heads * size
        model_width = pre_gain.shape[0]
        chunk = tokens.shape[1]
        cols = post_gain.shape[0]
        if cols % 128:
            out_w = jnp.moveaxis(out_weight.reshape(width, tp, cols), 1, 0)
        else:
            out_w = out_weight
        kept = jax.ShapeDtypeStruct if cols % 128 else pltpu.VMEM
        any_spec = pl.BlockSpec(memory_space=pltpu.HBM)
        vmem_spec = pl.BlockSpec(memory_space=pltpu.VMEM)
        dma = pltpu.SemaphoreType.DMA
        flat_rows = rows * heads
        mixed, committed = pl.pallas_call(
            functools.partial(layer_kernel, kv, tp, proposals, heads, model_width),
            out_shape=(
                kept((tokens.shape[0], cols), BF16),
                kept(saved_state.shape, F32),
            ),
            in_specs=[any_spec] * 18,
            out_specs=(vmem_spec, vmem_spec),
            scratch_shapes=[
                pltpu.VMEM(tokens.shape, BF16),
                pltpu.VMEM((kv, rows, chunk), BF16),
                pltpu.VMEM((4, kv, chunk, width), BF16),
                pltpu.VMEM((heads, seqs, size, size), BF16),
                pltpu.VMEM((tp, width, cols), BF16),
                pltpu.VMEM((4, rows, width), F32),
                pltpu.VMEM((rows, 2 * heads * tp), F32),
                pltpu.VMEM((heads, rows, size), BF16),
                pltpu.VMEM((2, kv, heads, rows, size), BF16),
                pltpu.VMEM((kv, rows, cols), F32),
                pltpu.VMEM((kv, tp, rows, cols), BF16),
                pltpu.VMEM((kv, tp, rows, cols), BF16),
                pltpu.VMEM((kv, rows), F32),
                pltpu.VMEM((kv * tp, kv, rows), F32),
                pltpu.VMEM((1, model_width), F32),
                pltpu.VMEM((heads * tp, model_width), BF16),
                pltpu.VMEM((heads * tp, model_width), BF16),
                pltpu.VMEM((1, heads), F32),
                pltpu.VMEM((1, size), F32),
                pltpu.VMEM((1, cols), F32),
                pltpu.VMEM((flat_rows, size), BF16),
                pltpu.VMEM((flat_rows, size), BF16),
                pltpu.VMEM((proposals, heads, seqs), F32),
                pltpu.VMEM((proposals, heads, seqs), F32),
                pltpu.VMEM((1, seqs), jnp.int32),
                dma((4, kv)), dma((flat_rows // min(128, flat_rows),)), dma((tp,)), dma, dma((11,)),
                dma((kv,)), dma((kv,)),
                dma((kv, tp)), dma((kv, tp)), dma((2, kv, heads)), dma((2, kv, heads)),
                dma((kv, tp)), dma((kv, tp)), dma((kv * tp,)), dma((kv * tp,)),
            ],
            compiler_params=pltpu.CompilerParams(
                collective_id=0, has_side_effects=True, vmem_limit_bytes=VMEM_BYTES * 5 // 3 if cols % 128 else VMEM_BYTES
            ),
            name="layer",
        )(*[pltpu.with_memory_space_constraint(x, pltpu.HBM) for x in (
            tokens, pre_gain.reshape(1, model_width), query_weight, key_weight, value_weight,
            gate_weight, beta_weight.T, decay_weight.T, decay_log.reshape(1, heads), head_gain.reshape(1, size), out_w,
            post_gain.reshape(1, cols), saved_state, earlier_keys.reshape(flat_rows, size),
            earlier_values.reshape(flat_rows, size), jnp.transpose(earlier_rates, (1, 2, 0)),
            jnp.transpose(earlier_decays, (1, 2, 0)), accepted.reshape(1, seqs),
        )])
        return (mixed, committed)

    return local


def solution(mesh):
    placed = (
        P("dp", "kv"),
        P(),
        P(None, "tp"),
        P(None, "tp"),
        P(None, "tp"),
        P(None, "tp"),
        P(),
        P(),
        P("tp"),
        P(),
        P("tp", "kv"),
        P(("kv", "tp")),
        P(("dp", "kv"), "tp", None, None),
        P(("dp", "kv"), None, "tp", None),
        P(("dp", "kv"), None, "tp", None),
        P(("dp", "kv"), None, "tp"),
        P(("dp", "kv"), None, "tp"),
        P(("dp", "kv")),
    )
    return jax.shard_map(
        make_local(mesh),
        mesh=mesh,
        in_specs=placed,
        out_specs=(P("dp", ("kv", "tp")), P(("dp", "kv"), "tp", None, None)),
        check_vma=False,
    )
```

```python
import functools

import jax
import jax.numpy as jnp
from jax import lax
from jax.experimental import pallas as pl
from jax.experimental.pallas import tpu as pltpu
from jax.sharding import PartitionSpec as P

F32 = jnp.float32
BF16 = jnp.bfloat16
EPS = 1e-06
MESH_IDS = pl.DeviceIdType.MESH
VMEM_BYTES = 36 * 1024 * 1024


def mm(a, b):
    return jnp.dot(a, b, preferred_element_type=F32)


def mm_nt(a, b):
    return lax.dot_general(a, b, (((1,), (1,)), ((), ())), preferred_element_type=F32)


def mm_tn(a, b):
    return lax.dot_general(a, b, (((0,), (0,)), ((), ())), preferred_element_type=F32)


def mm_exact(a, b):
    return jnp.dot(a, b, preferred_element_type=F32, precision=lax.Precision.HIGHEST)


def unit(values):
    return values * lax.rsqrt(jnp.sum(values * values, axis=-1, keepdims=True) + EPS)


def silu(values):
    return values / (1.0 + jnp.exp(-values))


def masks_of(rows, proposals):
    r = lax.broadcasted_iota(jnp.int32, (rows, rows), 0)
    c = lax.broadcasted_iota(jnp.int32, (rows, rows), 1)
    same = (r // proposals) == (c // proposals)
    return same, same & (c <= r), same & (c < r)


def per_sequence(operands, state_of, proposals, rows):
    size = operands[0].shape[1]
    group = 16
    seqs = group // proposals
    stack = group * len(operands)
    row = lax.broadcasted_iota(jnp.int32, (stack, size), 0)
    owner = (row % group) // proposals
    outs = [[] for _ in operands]
    for g in range(rows // group):
        x = jnp.concatenate([o[g * group:(g + 1) * group] for o in operands], axis=0)
        lhs = jnp.concatenate(
            [jnp.where(owner == s, x, 0.0).astype(BF16) for s in range(seqs)], axis=1
        )
        rhs = state_of(g * seqs, seqs).reshape(seqs * size, size).astype(BF16)
        y = mm(lhs, rhs)
        for i in range(len(operands)):
            outs[i].append(y[i * group:(i + 1) * group])
    return [jnp.concatenate(o, axis=0) for o in outs]


def solve(keys, values, recalled, rate, decay_pairs, gamma, strict):
    kb = keys.astype(BF16)
    low = (jnp.where(strict, decay_pairs * mm_nt(kb, kb), 0.0) * rate).astype(BF16)
    rhs = rate * (values - gamma * recalled)
    square = mm(low, low).astype(BF16)
    x = rhs + mm(square, rhs.astype(BF16))
    return x - mm(low, x.astype(BF16))


def head_masks(rows, group, heads):
    r = lax.broadcasted_iota(jnp.int32, (rows, rows), 0)
    c = lax.broadcasted_iota(jnp.int32, (rows, rows), 1)
    same = ((r // group) == (c // group)) & ((r % heads) == (c % heads))
    return same & (c <= r), same & (c < r)


def commit_table(proposals, heads, rates, decays, accepted):
    seqs = accepted.shape[1]
    live = [accepted > p for p in range(proposals)]
    rate = jnp.concatenate([jnp.where(live[p], rates[p], 0.0) for p in range(proposals)], axis=0)
    sums = [jnp.where(live[0], decays[0], 0.0)]
    for p in range(1, proposals):
        sums.append(sums[-1] + jnp.where(live[p], decays[p], 0.0))
    cum = jnp.concatenate(sums, axis=0)
    last = jnp.concatenate([sums[-1]] * proposals, axis=0)
    used = 3 * proposals * heads
    table = jnp.concatenate([rate, cum, last], axis=0)
    table = jnp.concatenate([table, jnp.zeros((used, 128 - seqs), F32)], axis=1)
    table = jnp.concatenate([table, jnp.zeros((128 - used, 128), F32)], axis=0)
    return table.T


def commit_block(block, proposals, heads, table, keys_raw, values, masks, com, sbf):
    rows, size = keys_raw.shape
    group = proposals * heads
    seqs = rows // group
    incl, strict = masks
    spread = jnp.concatenate(
        [
            jnp.broadcast_to(table[block * seqs + i:block * seqs + i + 1, :], (group, 128))
            for i in range(seqs)
        ],
        axis=0,
    )
    lane = lax.broadcasted_iota(jnp.int32, (rows, 128), 1)
    slot = lax.broadcasted_iota(jnp.int32, (rows, 128), 0) % group

    def column(k):
        return jnp.sum(jnp.where(lane == k * group + slot, spread, 0.0), axis=1, keepdims=True)

    rate, g_col, g_last = column(0), column(1), column(2)
    g_row = jnp.broadcast_to(g_col, (rows, rows)).T
    pairs = jnp.exp(jnp.where(incl, g_col - g_row, -1e30))
    keys = unit(keys_raw.astype(F32))
    owner = lax.broadcasted_iota(jnp.int32, (group, size), 0) % heads

    def widen(x):
        return jnp.concatenate(
            [jnp.where(owner == h, x, 0.0).astype(BF16) for h in range(heads)], axis=1
        )

    recalled = jnp.concatenate(
        [
            mm(
                widen(keys[i * group:(i + 1) * group]),
                com[block * seqs + i].reshape(heads * size, size).astype(BF16),
            )
            for i in range(seqs)
        ],
        axis=0,
    )
    w = solve(keys, values.astype(F32), recalled, rate, pairs, jnp.exp(g_col), strict)
    scaled_keys = (keys * jnp.exp(g_last - g_col)).astype(BF16)
    whole = jnp.broadcast_to(jnp.exp(g_last), (rows, size))
    for i in range(seqs):
        seq = block * seqs + i
        span = slice(i * group, (i + 1) * group)
        add = mm_tn(scaled_keys[span], widen(w[span]))
        for h in range(heads):
            keep = whole[i * group + h:i * group + h + 1]
            new = keep * com[seq, h] + add[:, h * size:(h + 1) * size]
            com[seq, h] = new
            sbf[h, seq] = new.astype(BF16)


def layer_kernel(
    kv, tp, proposals, heads, model_width,
    tokens, gains_h, qw, kw, vw, gw, beta_h, decay_h, log_h, head_gain_h, ow, post_h, state,
    ekeys_h, evalues_h, erates_h, edecays_h, accepted_h,
    out, com,
    tokv, tok, wv, sbf, owv, acc, sacc, att, passed, part, give, take, sums, sumall,
    gains, beta_t, decay_t, log_rate, head_gain, post, ekeys, evalues, erates, edecays, accepted,
    w_sem, s_sem, ow_sem, own_sem, small_sem, tok_send, tok_recv, half_send, half_recv,
    att_send, att_recv, tp_send, tp_recv, sum_send, sum_recv,
):
    me = lax.axis_index("kv")
    core = lax.axis_index("tp")
    rows, chunk = tok.shape[1], tok.shape[2]
    size = head_gain.shape[1]
    cols = out.shape[1]
    weights = (qw, kw, vw, gw)

    more_left = lax.div(2 * me, kv)
    both = more_left * (kv - 1 - me) + (1 - more_left) * me

    def nearest(j):
        if j == 0:
            return me
        paired = lax.div(2 * both - j + kv, kv)
        turned = me - (j + 1) // 2 if j % 2 else me + j // 2
        beyond = me + (1 - 2 * more_left) * (j - both)
        return paired * turned + (1 - paired) * beyond

    barrier = pltpu.get_barrier_semaphore()
    group = kv * tp
    flat = me * tp + core

    def peer(o):
        other = lax.rem(flat + o, group)
        return {"kv": other // tp, "tp": lax.rem(other, tp)}

    for o in range(1, group):
        pl.semaphore_signal(barrier, inc=1, device_id=peer(o), device_id_type=MESH_IDS)

    local = {}
    local["tok"] = pltpu.make_async_copy(tokens, tokv, own_sem)
    local["tok"].start()
    pairs_small = (
        (ekeys_h, ekeys), (evalues_h, evalues), (erates_h, erates), (edecays_h, edecays),
        (accepted_h, accepted), (gains_h, gains), (beta_h, beta_t), (decay_h, decay_t),
        (log_h, log_rate), (head_gain_h, head_gain), (post_h, post),
    )
    for i, (src, dst) in enumerate(pairs_small):
        local["small", i] = pltpu.make_async_copy(src, dst, small_sem.at[i])
        local["small", i].start()
    local["tok"].wait()
    block_rows = min(128, ekeys.shape[0])
    blocks_n = ekeys.shape[0] // block_rows
    block_seqs = state.shape[0] // blocks_n
    for b in range(blocks_n):
        span = pl.ds(b * block_seqs, block_seqs)
        local["s", b] = pltpu.make_async_copy(state.at[span], com.at[span], s_sem.at[b])
        local["s", b].start()

    def fetch_weights(d):
        c = nearest(d)
        for i in range(4):
            local["w", i, d] = pltpu.make_async_copy(
                weights[i].at[pl.ds(c * chunk, chunk), :], wv.at[i, d], w_sem.at[i, d]
            )
            local["w", i, d].start()

    for o in range(tp):
        half = lax.rem(core + o, tp)
        if len(ow.shape) == 3:
            src = ow.at[half]
        else:
            src = ow.at[:, pl.ds(pl.multiple_of(half * cols, 128), cols)]
        local["o", o] = pltpu.make_async_copy(src, owv.at[o], ow_sem.at[o])
        local["o", o].start()

    pl.semaphore_wait(barrier, group - 1)

    part_rows = rows // tp
    mine_rows = pl.ds(pl.multiple_of(core * part_rows, part_rows), part_rows)
    sent = {}
    halves = {}
    for d in range(kv - 1, 0, -1):
        c = nearest(d)
        sent[d] = pltpu.make_async_remote_copy(
            src_ref=tokv.at[
                pl.ds(pl.multiple_of(c * rows + core * part_rows, part_rows), part_rows), :
            ],
            dst_ref=tok.at[me, mine_rows],
            send_sem=tok_send.at[c],
            recv_sem=tok_recv.at[me],
            device_id={"kv": c},
            device_id_type=MESH_IDS,
        )
        sent[d].start()

    def arrival(d):
        c = nearest(d)
        return pltpu.make_async_remote_copy(
            src_ref=tok.at[c, mine_rows],
            dst_ref=tok.at[c, mine_rows],
            send_sem=tok_send.at[c],
            recv_sem=tok_recv.at[c],
            device_id={"kv": c},
            device_id_type=MESH_IDS,
        )

    def hand_over(d):
        c = nearest(d)
        arrival(d).wait_recv()
        for o in range(1, tp):
            halves[d, o] = pltpu.make_async_remote_copy(
                src_ref=tok.at[c, mine_rows],
                dst_ref=tok.at[c, mine_rows],
                send_sem=half_send.at[d, o],
                recv_sem=half_recv.at[d, o],
                device_id={"tp": lax.rem(core + o, tp)},
                device_id_type=MESH_IDS,
            )
            halves[d, o].start()

    def project(d, squares):
        if d > 0:
            for o in range(1, tp):
                halves[d, o].wait_recv()
        c = nearest(d)
        span = pl.ds(pl.multiple_of(c * chunk, 128), chunk)
        if d == 0:
            wide = tokv[pl.ds(pl.multiple_of(me * rows, rows), rows), :].astype(F32)
        else:
            wide = tok[c].astype(F32)
        scaled = (wide * gains[:, span]).astype(BF16)
        thin = mm_nt(scaled, jnp.concatenate([beta_t[:, span], decay_t[:, span]], axis=0))
        if d == 0:
            sacc[...] = thin
        else:
            sacc[...] += thin
        for i in range(4):
            local["w", i, d].wait()
            y = mm(scaled, wv[i, d])
            if d == 0:
                acc[i] = y
            else:
                acc[i] += y
        return squares + jnp.sum(wide * wide, axis=1, keepdims=True)

    for i in range(len(pairs_small)):
        local["small", i].wait()
    table = commit_table(proposals, heads, erates[...], edecays[...], accepted[...])
    commit_masks = head_masks(block_rows, proposals * heads, heads)
    squares = jnp.zeros((rows, 1), F32)
    for b in range(blocks_n):
        span = slice(b * block_rows, (b + 1) * block_rows)
        local["s", b].wait()
        for d in range(b * kv // blocks_n, (b + 1) * kv // blocks_n):
            fetch_weights(d)
        commit_block(
            b, proposals, heads, table, ekeys[span], evalues[span], commit_masks, com, sbf
        )
    squares = project(0, squares)
    for d in range(1, kv):
        hand_over(d)
        if d > 1:
            squares = project(d - 1, squares)
    if kv > 1:
        squares = project(kv - 1, squares)
    inverse = lax.rsqrt(squares / model_width + EPS)

    same, incl, strict = masks_of(rows, proposals)
    all_heads = heads * tp
    pad = jnp.zeros((rows, 128 - 2 * all_heads), F32)
    raw = jnp.concatenate([sacc[...] * inverse, pad], axis=1)
    raw = pltpu.roll(raw, lax.rem(128 - core * heads, 128), axis=1)
    rates = 1.0 / (1.0 + jnp.exp(-raw))
    soft = jnp.maximum(raw, 0.0) + jnp.log1p(jnp.exp(-jnp.abs(raw)))
    speed = jnp.concatenate(
        [
            jnp.zeros((1, all_heads), F32), jnp.exp(log_rate[...]),
            jnp.zeros((1, 128 - all_heads - heads), F32),
        ],
        axis=1,
    )
    cum = -speed * soft
    place = lax.broadcasted_iota(jnp.int32, (rows, 128), 0) % proposals
    step = 1
    while step < proposals:
        cum = cum + jnp.where(place >= step, pltpu.roll(cum, step, axis=0), 0.0)
        step *= 2
    cum_t = cum.T

    def parent(s):
        return s - 1 if s % 2 else s - 2

    def hop(way, s, h):
        step = s - parent(s)
        if way:
            step = kv - step
        return pltpu.make_async_remote_copy(
            src_ref=att.at[h] if parent(s) == 0 else passed.at[way, parent(s), h],
            dst_ref=passed.at[way, s, h],
            send_sem=att_send.at[way, s, h],
            recv_sem=att_recv.at[way, s, h],
            device_id={"kv": lax.rem(me + step, kv)},
            device_id_type=MESH_IDS,
        )

    def arrives(way, s):
        return me - s >= 0 if way == 0 else me + s < kv

    def leaves(way, reach):
        return me + reach < kv if way == 0 else me >= reach

    def children(s):
        return [t for t in (s + 2, s + 1) if t < kv]

    lag = 3

    def relays(s):
        return s % 2 == 0 and bool(children(s))

    def advance(turn):
        for s in range(0, kv, 2):
            h = turn - lag * (s // 2)
            if not 0 <= h < heads or not relays(s):
                continue
            for way in range(2):
                if s > 0:
                    @pl.when(arrives(way, s) & leaves(way, 1))
                    def _():
                        hop(way, s, h).wait_recv()
                for t in children(s):
                    @pl.when(arrives(way, s) & leaves(way, t - s))
                    def _():
                        hop(way, t, h).start()

    def gather(way, s):
        if way is None:
            return
        here = arrives(way, s)
        if relays(s):
            here = here & jnp.logical_not(leaves(way, 1))

        @pl.when(here)
        def _():
            for h in range(heads):
                hop(way, s, h).wait_recv()

    def settle():
        for s in range(0, kv, 2):
            for t in children(s):
                for way in range(2):
                    @pl.when(arrives(way, s) & leaves(way, t - s))
                    def _():
                        for h in range(heads):
                            hop(way, t, h).wait_send()

    for first in range(heads):
        batch = range(first, first + 1)
        query, key, pairs, gamma, w, asked, reads = {}, {}, {}, {}, {}, {}, {}
        recalled = {}
        for h in batch:
            block = slice(h * size, (h + 1) * size)
            query[h] = unit(silu(acc[0, :, block] * inverse)) * size ** (-0.5)
            key[h] = unit(silu(acc[1, :, block] * inverse))
            pairs[h] = jnp.exp(jnp.where(incl, cum[:, all_heads + h:all_heads + h + 1] - cum_t[all_heads + h:all_heads + h + 1, :], -1e30))
            gamma[h] = jnp.exp(cum[:, all_heads + h:all_heads + h + 1])
        for h in batch:
            recalled[h], asked[h] = per_sequence(
                [key[h], query[h]], lambda s, n, h=h: sbf[h, s:s + n], proposals, rows
            )
        for h in batch:
            value = silu(acc[2, :, h * size:(h + 1) * size] * inverse)
            w[h] = solve(key[h], value, recalled[h], rates[:, h:h + 1], pairs[h], gamma[h], strict)
        for h in batch:
            mix = (pairs[h] * mm_nt(query[h].astype(BF16), key[h].astype(BF16))).astype(BF16)
            reads[h] = gamma[h] * asked[h] + mm(mix, w[h].astype(BF16))
        for h in batch:
            gate = silu(acc[3, :, h * size:(h + 1) * size] * inverse)
            scale = lax.rsqrt(jnp.mean(reads[h] * reads[h], axis=-1, keepdims=True) + EPS)
            att[h] = (reads[h] * scale * head_gain[...] * gate).astype(BF16)
        for h in batch:
            advance(h)

    for o in range(tp):
        local["o", o].wait()

    def swap(c, o):
        return pltpu.make_async_remote_copy(
            src_ref=give.at[c, o],
            dst_ref=take.at[c, o],
            send_sem=tp_send.at[c, o],
            recv_sem=tp_recv.at[c, o],
            device_id={"tp": lax.rem(core + o, tp)},
            device_id_type=MESH_IDS,
        )

    def combine(c, pieces):
        rows_in = jnp.concatenate(pieces, axis=1)
        for o in range(1, tp):
            give[c, o] = mm(rows_in, owv[o]).astype(BF16)
            swap(c, o).start()
        part[c] = mm(rows_in, owv[0])

    def finish(c):
        own = part[c]
        for o in range(1, tp):
            swap(c, o).wait_recv()
            own = own + take[c, o].astype(F32)
        part[c] = own
        total = jnp.sum(own * own, axis=1, keepdims=True)
        sums[pl.ds(c, 1), :] = jnp.broadcast_to(total, (rows, rows)).T[0:1]

    def blocks(s):
        if s == 0:
            return [(True, me, None)]
        return [(arrives(way, s), me - s if way == 0 else me + s, way) for way in range(2)]

    def finish_at(s):
        if s == 0:
            finish(me)
            return
        for here, c, way in blocks(s):
            @pl.when(here)
            def _():
                finish(c)

    deepest = max([s for s in range(kv) if relays(s)], default=0)
    for turn in range(heads, heads + lag * (deepest // 2)):
        advance(turn)
        if turn == heads:
            combine(me, [att[h] for h in range(heads)])
    if not deepest:
        combine(me, [att[h] for h in range(heads)])
    for s in range(1, kv):
        for here, c, way in blocks(s):
            gather(way, s)

            @pl.when(here)
            def _():
                combine(c, [passed[way, s, h] for h in range(heads)])
        finish_at(s - 1)
    finish_at(kv - 1)
    tells = {}
    for o in range(1, group):
        tells[o] = pltpu.make_async_remote_copy(
            src_ref=sums,
            dst_ref=sumall.at[o],
            send_sem=sum_send.at[o],
            recv_sem=sum_recv.at[o],
            device_id=peer(o),
            device_id_type=MESH_IDS,
        )
        tells[o].start()
    totals = sums[...]
    for o in range(1, group):
        tells[o].wait_recv()
        totals = totals + sumall[o]
    sums_factor = lax.rsqrt(totals / model_width + EPS)
    for o in range(1, group):
        tells[o].wait_send()
    settle()
    for d in range(1, kv):
        sent[d].wait_send()
        for o in range(1, tp):
            halves[d, o].wait_send()
    for c in range(kv):
        for o in range(1, tp):
            swap(c, o).wait_send()
    for c in range(kv):
        factor = jnp.broadcast_to(sums_factor[c:c + 1, :], (rows, rows)).T[:, 0:1]
        out[c * rows:(c + 1) * rows, :] = (part[c] * factor * post[...]).astype(BF16)


def make_local(mesh):
    kv = mesh.shape["kv"]
    tp = mesh.shape["tp"]

    def local(
        tokens, pre_gain, query_weight, key_weight, value_weight, gate_weight, beta_weight,
        decay_weight, decay_log, head_gain, out_weight, post_gain, saved_state, earlier_keys,
        earlier_values, earlier_rates, earlier_decays, accepted,
    ):
        seqs, heads, size = saved_state.shape[:3]
        proposals = earlier_keys.shape[1]
        rows = seqs * proposals
        width = heads * size
        model_width = pre_gain.shape[0]
        chunk = tokens.shape[1]
        cols = post_gain.shape[0]
        if cols % 128:
            out_w = jnp.moveaxis(out_weight.reshape(width, tp, cols), 1, 0)
        else:
            out_w = out_weight
        kept = jax.ShapeDtypeStruct if cols % 128 else pltpu.VMEM
        any_spec = pl.BlockSpec(memory_space=pltpu.HBM)
        vmem_spec = pl.BlockSpec(memory_space=pltpu.VMEM)
        dma = pltpu.SemaphoreType.DMA
        flat_rows = rows * heads
        mixed, committed = pl.pallas_call(
            functools.partial(layer_kernel, kv, tp, proposals, heads, model_width),
            out_shape=(
                kept((tokens.shape[0], cols), BF16),
                kept(saved_state.shape, F32),
            ),
            in_specs=[any_spec] * 18,
            out_specs=(vmem_spec, vmem_spec),
            scratch_shapes=[
                pltpu.VMEM(tokens.shape, BF16),
                pltpu.VMEM((kv, rows, chunk), BF16),
                pltpu.VMEM((4, kv, chunk, width), BF16),
                pltpu.VMEM((heads, seqs, size, size), BF16),
                pltpu.VMEM((tp, width, cols), BF16),
                pltpu.VMEM((4, rows, width), F32),
                pltpu.VMEM((rows, 2 * heads * tp), F32),
                pltpu.VMEM((heads, rows, size), BF16),
                pltpu.VMEM((2, kv, heads, rows, size), BF16),
                pltpu.VMEM((kv, rows, cols), F32),
                pltpu.VMEM((kv, tp, rows, cols), BF16),
                pltpu.VMEM((kv, tp, rows, cols), BF16),
                pltpu.VMEM((kv, rows), F32),
                pltpu.VMEM((kv * tp, kv, rows), F32),
                pltpu.VMEM((1, model_width), F32),
                pltpu.VMEM((heads * tp, model_width), BF16),
                pltpu.VMEM((heads * tp, model_width), BF16),
                pltpu.VMEM((1, heads), F32),
                pltpu.VMEM((1, size), F32),
                pltpu.VMEM((1, cols), F32),
                pltpu.VMEM((flat_rows, size), BF16),
                pltpu.VMEM((flat_rows, size), BF16),
                pltpu.VMEM((proposals, heads, seqs), F32),
                pltpu.VMEM((proposals, heads, seqs), F32),
                pltpu.VMEM((1, seqs), jnp.int32),
                dma((4, kv)), dma((flat_rows // min(128, flat_rows),)), dma((tp,)), dma, dma((11,)),
                dma((kv,)), dma((kv,)),
                dma((kv, tp)), dma((kv, tp)), dma((2, kv, heads)), dma((2, kv, heads)),
                dma((kv, tp)), dma((kv, tp)), dma((kv * tp,)), dma((kv * tp,)),
            ],
            compiler_params=pltpu.CompilerParams(
                collective_id=0, has_side_effects=True, vmem_limit_bytes=VMEM_BYTES * 5 // 3 if cols % 128 else VMEM_BYTES
            ),
            name="layer",
        )(*[pltpu.with_memory_space_constraint(x, pltpu.HBM) for x in (
            tokens, pre_gain.reshape(1, model_width), query_weight, key_weight, value_weight,
            gate_weight, beta_weight.T, decay_weight.T, decay_log.reshape(1, heads), head_gain.reshape(1, size), out_w,
            post_gain.reshape(1, cols), saved_state, earlier_keys.reshape(flat_rows, size),
            earlier_values.reshape(flat_rows, size), jnp.transpose(earlier_rates, (1, 2, 0)),
            jnp.transpose(earlier_decays, (1, 2, 0)), accepted.reshape(1, seqs),
        )])
        return (mixed, committed)

    return local


def solution(mesh):
    placed = (
        P("dp", "kv"),
        P(),
        P(None, "tp"),
        P(None, "tp"),
        P(None, "tp"),
        P(None, "tp"),
        P(),
        P(),
        P("tp"),
        P(),
        P("tp", "kv"),
        P(("kv", "tp")),
        P(("dp", "kv"), "tp", None, None),
        P(("dp", "kv"), None, "tp", None),
        P(("dp", "kv"), None, "tp", None),
        P(("dp", "kv"), None, "tp"),
        P(("dp", "kv"), None, "tp"),
        P(("dp", "kv")),
    )
    return jax.shard_map(
        make_local(mesh),
        mesh=mesh,
        in_specs=placed,
        out_specs=(P("dp", ("kv", "tp")), P(("dp", "kv"), "tp", None, None)),
        check_vma=False,
    )
```

```python
import functools
import math

import jax
import jax.numpy as jnp
from jax import lax
from jax.experimental import pallas as pl
from jax.experimental.pallas import tpu as pltpu
from jax.sharding import PartitionSpec as P

F32 = jnp.float32
BF16 = jnp.bfloat16
EPS = 1e-06
MESH_IDS = pl.DeviceIdType.MESH
VMEM_BYTES = 36 * 1024 * 1024


def mm(a, b):
    return jnp.dot(a, b, preferred_element_type=F32)


def mm_nt(a, b):
    return lax.dot_general(a, b, (((1,), (1,)), ((), ())), preferred_element_type=F32)


def mm_tn(a, b):
    return lax.dot_general(a, b, (((0,), (0,)), ((), ())), preferred_element_type=F32)


def mm_exact(a, b):
    return jnp.dot(a, b, preferred_element_type=F32, precision=lax.Precision.HIGHEST)


def unit(values):
    return values * lax.rsqrt(jnp.sum(values * values, axis=-1, keepdims=True) + EPS)


def silu(values):
    return values / (1.0 + jnp.exp(-values))


def masks_of(rows, proposals):
    r = lax.broadcasted_iota(jnp.int32, (rows, rows), 0)
    c = lax.broadcasted_iota(jnp.int32, (rows, rows), 1)
    same = (r // proposals) == (c // proposals)
    return same, same & (c <= r), same & (c < r)


def per_sequence(operands, state_of, proposals, rows):
    size = operands[0].shape[1]
    group = 16
    seqs = group // proposals
    stack = group * len(operands)
    row = lax.broadcasted_iota(jnp.int32, (stack, size), 0)
    owner = (row % group) // proposals
    outs = [[] for _ in operands]
    for g in range(rows // group):
        x = jnp.concatenate([o[g * group:(g + 1) * group] for o in operands], axis=0)
        lhs = jnp.concatenate(
            [jnp.where(owner == s, x, 0.0).astype(BF16) for s in range(seqs)], axis=1
        )
        rhs = state_of(g * seqs, seqs).reshape(seqs * size, size).astype(BF16)
        y = mm(lhs, rhs)
        for i in range(len(operands)):
            outs[i].append(y[i * group:(i + 1) * group])
    return [jnp.concatenate(o, axis=0) for o in outs]


def solve(keys, values, recalled, rate, decay_pairs, gamma, strict):
    kb = keys.astype(BF16)
    low = (jnp.where(strict, decay_pairs * mm_nt(kb, kb), 0.0) * rate).astype(BF16)
    rhs = rate * (values - gamma * recalled)
    square = mm(low, low).astype(BF16)
    x = rhs + mm(square, rhs.astype(BF16))
    return x - mm(low, x.astype(BF16))


def head_masks(rows, group, heads):
    r = lax.broadcasted_iota(jnp.int32, (rows, rows), 0)
    c = lax.broadcasted_iota(jnp.int32, (rows, rows), 1)
    same = ((r // group) == (c // group)) & ((r % heads) == (c % heads))
    return same & (c <= r), same & (c < r)


def commit_table(proposals, heads, rates, decays, accepted):
    seqs = accepted.shape[1]
    live = [accepted > p for p in range(proposals)]
    rate = jnp.concatenate([jnp.where(live[p], rates[p], 0.0) for p in range(proposals)], axis=0)
    sums = [jnp.where(live[0], decays[0], 0.0)]
    for p in range(1, proposals):
        sums.append(sums[-1] + jnp.where(live[p], decays[p], 0.0))
    cum = jnp.concatenate(sums, axis=0)
    last = jnp.concatenate([sums[-1]] * proposals, axis=0)
    used = 3 * proposals * heads
    table = jnp.concatenate([rate, cum, last], axis=0)
    table = jnp.concatenate([table, jnp.zeros((used, 128 - seqs), F32)], axis=1)
    table = jnp.concatenate([table, jnp.zeros((128 - used, 128), F32)], axis=0)
    return table.T


def commit_block(block, proposals, heads, table, keys_raw, values, masks, com, sbf):
    rows, size = keys_raw.shape
    group = proposals * heads
    seqs = rows // group
    incl, strict = masks
    spread = jnp.concatenate(
        [
            jnp.broadcast_to(table[block * seqs + i:block * seqs + i + 1, :], (group, 128))
            for i in range(seqs)
        ],
        axis=0,
    )
    lane = lax.broadcasted_iota(jnp.int32, (rows, 128), 1)
    slot = lax.broadcasted_iota(jnp.int32, (rows, 128), 0) % group

    def column(k):
        return jnp.sum(jnp.where(lane == k * group + slot, spread, 0.0), axis=1, keepdims=True)

    rate, g_col, g_last = column(0), column(1), column(2)
    g_row = jnp.broadcast_to(g_col, (rows, rows)).T
    pairs = jnp.exp(jnp.where(incl, g_col - g_row, -1e30))
    keys = unit(keys_raw.astype(F32))
    owner = lax.broadcasted_iota(jnp.int32, (group, size), 0) % heads

    def widen(x):
        return jnp.concatenate(
            [jnp.where(owner == h, x, 0.0).astype(BF16) for h in range(heads)], axis=1
        )

    recalled = jnp.concatenate(
        [
            mm(
                widen(keys[i * group:(i + 1) * group]),
                com[block * seqs + i].reshape(heads * size, size).astype(BF16),
            )
            for i in range(seqs)
        ],
        axis=0,
    )
    w = solve(keys, values.astype(F32), recalled, rate, pairs, jnp.exp(g_col), strict)
    scaled_keys = (keys * jnp.exp(g_last - g_col)).astype(BF16)
    whole = jnp.broadcast_to(jnp.exp(g_last), (rows, size))
    for i in range(seqs):
        seq = block * seqs + i
        span = slice(i * group, (i + 1) * group)
        add = mm_tn(scaled_keys[span], widen(w[span]))
        for h in range(heads):
            keep = whole[i * group + h:i * group + h + 1]
            new = keep * com[seq, h] + add[:, h * size:(h + 1) * size]
            com[seq, h] = new
            sbf[h, seq] = new.astype(BF16)


def layer_kernel(
    kv, tp, proposals, heads, model_width,
    tokens, gains_h, qw, kw, vw, gw, beta_h, decay_h, log_h, head_gain_h, ow, post_h, state,
    ekeys_h, evalues_h, erates_h, edecays_h, accepted_h,
    part, factors, com,
    tokv, tok, wv, sbf, owv, acc, sacc, att, passed, give, take, sums, sumall,
    gains, beta_t, decay_t, log_rate, head_gain, post, ekeys, evalues, erates, edecays, accepted,
    w_sem, s_sem, ow_sem, own_sem, small_sem, tok_send, tok_recv, half_send, half_recv,
    att_send, att_recv, tp_send, tp_recv, sum_send, sum_recv,
):
    me = lax.axis_index("kv")
    core = lax.axis_index("tp")
    rows, chunk = tok.shape[1], tok.shape[2]
    size = head_gain.shape[1]
    cols = part.shape[2]
    weights = (qw, kw, vw, gw)

    more_left = lax.div(2 * me, kv)
    both = more_left * (kv - 1 - me) + (1 - more_left) * me

    def nearest(j):
        paired = lax.div(2 * both - j + kv, kv)
        turned = me + (1 - 2 * (j % 2)) * ((j + 1) // 2)
        beyond = me + (1 - 2 * more_left) * (j - both)
        return paired * turned + (1 - paired) * beyond

    barrier = pltpu.get_barrier_semaphore()
    group = kv * tp
    flat = me * tp + core

    def peer(o):
        other = lax.rem(flat + o, group)
        return {"kv": other // tp, "tp": lax.rem(other, tp)}

    for o in range(1, group):
        pl.semaphore_signal(barrier, inc=1, device_id=peer(o), device_id_type=MESH_IDS)

    local = {}
    local["tok"] = pltpu.make_async_copy(tokens, tokv, own_sem)
    local["tok"].start()
    pairs_small = (
        (ekeys_h, ekeys), (evalues_h, evalues), (erates_h, erates), (edecays_h, edecays),
        (accepted_h, accepted), (gains_h, gains), (beta_h, beta_t), (decay_h, decay_t),
        (log_h, log_rate), (head_gain_h, head_gain), (post_h, post),
    )
    for i, (src, dst) in enumerate(pairs_small):
        local["small", i] = pltpu.make_async_copy(src, dst, small_sem.at[i])
        local["small", i].start()
    local["tok"].wait()
    block_rows = min(128, ekeys.shape[0])
    blocks_n = ekeys.shape[0] // block_rows
    block_seqs = state.shape[0] // blocks_n
    for b in range(blocks_n):
        span = pl.ds(b * block_seqs, block_seqs)
        local["s", b] = pltpu.make_async_copy(state.at[span], com.at[span], s_sem.at[b])
        local["s", b].start()

    def fetch_weights(d):
        c = nearest(d)
        for i in range(4):
            local["w", i, d] = pltpu.make_async_copy(
                weights[i].at[pl.ds(c * chunk, chunk), :], wv.at[i, d], w_sem.at[i, d]
            )
            local["w", i, d].start()

    for o in range(tp):
        half = lax.rem(core + o, tp)
        if len(ow.shape) == 3:
            src = ow.at[half]
        else:
            src = ow.at[:, pl.ds(pl.multiple_of(half * cols, 128), cols)]
        local["o", o] = pltpu.make_async_copy(src, owv.at[o], ow_sem.at[o])
        local["o", o].start()

    pl.semaphore_wait(barrier, group - 1)

    part_rows = rows // tp
    mine_rows = pl.ds(pl.multiple_of(core * part_rows, part_rows), part_rows)
    sent = {}
    halves = {}
    for d in range(1, kv):
        c = nearest(d)
        sent[d] = pltpu.make_async_remote_copy(
            src_ref=tokv.at[
                pl.ds(pl.multiple_of(c * rows + core * part_rows, part_rows), part_rows), :
            ],
            dst_ref=tok.at[me, mine_rows],
            send_sem=tok_send.at[c],
            recv_sem=tok_recv.at[me],
            device_id={"kv": c},
            device_id_type=MESH_IDS,
        )
        sent[d].start()

    def arrival(d):
        c = nearest(d)
        return pltpu.make_async_remote_copy(
            src_ref=tok.at[c, mine_rows],
            dst_ref=tok.at[c, mine_rows],
            send_sem=tok_send.at[c],
            recv_sem=tok_recv.at[c],
            device_id={"kv": c},
            device_id_type=MESH_IDS,
        )

    def hand_over(d):
        c = nearest(d)
        arrival(d).wait_recv()
        for o in range(1, tp):
            halves[d, o] = pltpu.make_async_remote_copy(
                src_ref=tok.at[c, mine_rows],
                dst_ref=tok.at[c, mine_rows],
                send_sem=half_send.at[d, o],
                recv_sem=half_recv.at[d, o],
                device_id={"tp": lax.rem(core + o, tp)},
                device_id_type=MESH_IDS,
            )
            halves[d, o].start()

    def project(d, squares):
        if d > 0:
            for o in range(1, tp):
                halves[d, o].wait_recv()
        c = nearest(d)
        span = pl.ds(pl.multiple_of(c * chunk, 128), chunk)
        if d == 0:
            wide = tokv[pl.ds(pl.multiple_of(me * rows, rows), rows), :].astype(F32)
        else:
            wide = tok[c].astype(F32)
        scaled = (wide * gains[:, span]).astype(BF16)
        thin = mm_nt(scaled, jnp.concatenate([beta_t[:, span], decay_t[:, span]], axis=0))
        if d == 0:
            sacc[...] = thin
        else:
            sacc[...] += thin
        for i in range(4):
            local["w", i, d].wait()
            y = mm(scaled, wv[i, d])
            if d == 0:
                acc[i] = y
            else:
                acc[i] += y
        return squares + jnp.sum(wide * wide, axis=1, keepdims=True)

    for i in range(len(pairs_small)):
        local["small", i].wait()
    table = commit_table(proposals, heads, erates[...], edecays[...], accepted[...])
    commit_masks = head_masks(block_rows, proposals * heads, heads)
    squares = jnp.zeros((rows, 1), F32)
    for b in range(blocks_n):
        span = slice(b * block_rows, (b + 1) * block_rows)
        local["s", b].wait()
        for d in range(b * kv // blocks_n, (b + 1) * kv // blocks_n):
            fetch_weights(d)
        commit_block(
            b, proposals, heads, table, ekeys[span], evalues[span], commit_masks, com, sbf
        )
    for d in range(1, kv):
        hand_over(d)
        squares = project(d - 1, squares)
    squares = project(kv - 1, squares)
    inverse = lax.rsqrt(squares / model_width + EPS)

    same, incl, strict = masks_of(rows, proposals)
    all_heads = heads * tp
    pad = jnp.zeros((rows, 128 - 2 * all_heads), F32)
    raw = jnp.concatenate([sacc[...] * inverse, pad], axis=1)
    raw = pltpu.roll(raw, lax.rem(128 - core * heads, 128), axis=1)
    rates = 1.0 / (1.0 + jnp.exp(-raw))
    soft = jnp.maximum(raw, 0.0) + jnp.log1p(jnp.exp(-jnp.abs(raw)))
    speed = jnp.concatenate(
        [
            jnp.zeros((1, all_heads), F32), jnp.exp(log_rate[...]),
            jnp.zeros((1, 128 - all_heads - heads), F32),
        ],
        axis=1,
    )
    cum = -speed * soft
    place = lax.broadcasted_iota(jnp.int32, (rows, 128), 0) % proposals
    step = 1
    while step < proposals:
        cum = cum + jnp.where(place >= step, pltpu.roll(cum, step, axis=0), 0.0)
        step *= 2
    cum_t = cum.T

    stride = 2

    def parent(s):
        return (s - 1) // stride * stride

    def hop(way, s, h):
        step = s - parent(s)
        if way:
            step = kv - step
        return pltpu.make_async_remote_copy(
            src_ref=att.at[h] if parent(s) == 0 else passed.at[way, parent(s), h],
            dst_ref=passed.at[way, s, h],
            send_sem=att_send.at[way, s, h],
            recv_sem=att_recv.at[way, s, h],
            device_id={"kv": lax.rem(me + step, kv)},
            device_id_type=MESH_IDS,
        )

    def arrives(way, s):
        return me - s >= 0 if way == 0 else me + s < kv

    def leaves(way, reach):
        return me + reach < kv if way == 0 else me >= reach

    def children(s):
        return [t for t in range(s + stride, s, -1) if t < kv]

    lag = 3

    def relays(s):
        return s % stride == 0 and bool(children(s))

    def advance(turn):
        for s in range(0, kv, stride):
            h = turn - lag * (s // stride)
            if not 0 <= h < heads or not relays(s):
                continue
            for way in range(2):
                if s > 0:
                    @pl.when(arrives(way, s) & leaves(way, 1))
                    def _():
                        hop(way, s, h).wait_recv()
                for t in children(s):
                    @pl.when(arrives(way, s) & leaves(way, t - s))
                    def _():
                        hop(way, t, h).start()

    def gather(way, s):
        if way is None:
            return
        here = arrives(way, s)
        if relays(s):
            here = here & jnp.logical_not(leaves(way, 1))

        @pl.when(here)
        def _():
            for h in range(heads):
                hop(way, s, h).wait_recv()

    def settle():
        for s in range(0, kv, stride):
            for t in children(s):
                for way in range(2):
                    @pl.when(arrives(way, s) & leaves(way, t - s))
                    def _():
                        for h in range(heads):
                            hop(way, t, h).wait_send()

    for first in range(heads):
        batch = range(first, first + 1)
        query, key, pairs, gamma, w, asked, reads = {}, {}, {}, {}, {}, {}, {}
        recalled = {}
        for h in batch:
            block = slice(h * size, (h + 1) * size)
            query[h] = unit(silu(acc[0, :, block] * inverse)) * size ** (-0.5)
            key[h] = unit(silu(acc[1, :, block] * inverse))
            pairs[h] = jnp.exp(jnp.where(incl, cum[:, all_heads + h:all_heads + h + 1] - cum_t[all_heads + h:all_heads + h + 1, :], -1e30))
            gamma[h] = jnp.exp(cum[:, all_heads + h:all_heads + h + 1])
        for h in batch:
            recalled[h], asked[h] = per_sequence(
                [key[h], query[h]], lambda s, n, h=h: sbf[h, s:s + n], proposals, rows
            )
        for h in batch:
            value = silu(acc[2, :, h * size:(h + 1) * size] * inverse)
            w[h] = solve(key[h], value, recalled[h], rates[:, h:h + 1], pairs[h], gamma[h], strict)
        for h in batch:
            mix = (pairs[h] * mm_nt(query[h].astype(BF16), key[h].astype(BF16))).astype(BF16)
            reads[h] = gamma[h] * asked[h] + mm(mix, w[h].astype(BF16))
        for h in batch:
            gate = silu(acc[3, :, h * size:(h + 1) * size] * inverse)
            scale = lax.rsqrt(jnp.mean(reads[h] * reads[h], axis=-1, keepdims=True) + EPS)
            att[h] = (reads[h] * scale * head_gain[...] * gate).astype(BF16)
        for h in batch:
            advance(h)

    for o in range(tp):
        local["o", o].wait()

    def swap(c, o):
        return pltpu.make_async_remote_copy(
            src_ref=give.at[c, o],
            dst_ref=take.at[c, o],
            send_sem=tp_send.at[c, o],
            recv_sem=tp_recv.at[c, o],
            device_id={"tp": lax.rem(core + o, tp)},
            device_id_type=MESH_IDS,
        )

    def combine(c, pieces):
        rows_in = jnp.concatenate(pieces, axis=1)
        for o in range(1, tp):
            give[c, o] = mm(rows_in, owv[o]).astype(BF16)
            swap(c, o).start()
        part[c] = mm(rows_in, owv[0])

    def finish(c):
        own = part[c]
        for o in range(1, tp):
            swap(c, o).wait_recv()
            own = own + take[c, o].astype(F32)
        part[c] = own * post[...]
        total = jnp.sum(own * own, axis=1, keepdims=True)
        sums[pl.ds(c, 1), :] = jnp.broadcast_to(total, (rows, rows)).T[0:1]

    def blocks(s):
        if s == 0:
            return [(True, me, None)]
        return [(arrives(way, s), me - s if way == 0 else me + s, way) for way in range(2)]

    def finish_at(s):
        if s == 0:
            finish(me)
            return
        for here, c, way in blocks(s):
            @pl.when(here)
            def _():
                finish(c)

    deepest = max([s for s in range(kv) if relays(s)], default=0)
    for turn in range(heads, heads + lag * (deepest // stride)):
        advance(turn)
        if turn == heads:
            combine(me, [att[h] for h in range(heads)])
    if not deepest:
        combine(me, [att[h] for h in range(heads)])
    for s in range(1, kv):
        for here, c, way in blocks(s):
            gather(way, s)

            @pl.when(here)
            def _():
                combine(c, [passed[way, s, h] for h in range(heads)])
        finish_at(s - 1)
    finish_at(kv - 1)
    tells = {}
    for o in range(1, group):
        tells[o] = pltpu.make_async_remote_copy(
            src_ref=sums,
            dst_ref=sumall.at[o],
            send_sem=sum_send.at[o],
            recv_sem=sum_recv.at[o],
            device_id=peer(o),
            device_id_type=MESH_IDS,
        )
        tells[o].start()
    totals = sums[...]
    for o in range(1, group):
        tells[o].wait_recv()
        totals = totals + sumall[o]
    factors[...] = lax.rsqrt(totals / model_width + EPS)
    for o in range(1, group):
        tells[o].wait_send()
    settle()
    for d in range(1, kv):
        sent[d].wait_send()
        for o in range(1, tp):
            halves[d, o].wait_send()
    for c in range(kv):
        for o in range(1, tp):
            swap(c, o).wait_send()


def scale_rows(part, factors, mixed):
    kv, rows, cols = part.shape
    for c in range(kv):
        factor = jnp.broadcast_to(factors[c:c + 1, :], (rows, rows)).T[:, 0:1]
        mixed[c * rows:(c + 1) * rows, :] = (part[c] * factor).astype(BF16)


def store_kernel(pieces, part, factors, com, mixed_out, com_out, mixed, sems):
    copies = []
    size = com.shape[0] // pieces
    for i in range(pieces):
        span = pl.ds(i * size, size)
        copies.append(pltpu.make_async_copy(com.at[span], com_out.at[span], sems.at[i]))
    for copy in copies:
        copy.start()
    scale_rows(part, factors, mixed)
    copies.append(pltpu.make_async_copy(mixed, mixed_out, sems.at[pieces]))
    copies[-1].start()
    for copy in copies:
        copy.wait()


def make_local(mesh):
    kv = mesh.shape["kv"]
    tp = mesh.shape["tp"]

    def local(
        tokens, pre_gain, query_weight, key_weight, value_weight, gate_weight, beta_weight,
        decay_weight, decay_log, head_gain, out_weight, post_gain, saved_state, earlier_keys,
        earlier_values, earlier_rates, earlier_decays, accepted,
    ):
        seqs, heads, size = saved_state.shape[:3]
        proposals = earlier_keys.shape[1]
        rows = seqs * proposals
        width = heads * size
        model_width = pre_gain.shape[0]
        chunk = tokens.shape[1]
        cols = post_gain.shape[0]
        if cols % 128:
            out_w = jnp.moveaxis(out_weight.reshape(width, tp, cols), 1, 0)
        else:
            out_w = out_weight
        kept = jax.ShapeDtypeStruct if cols % 128 else pltpu.VMEM
        any_spec = pl.BlockSpec(memory_space=pltpu.HBM)
        vmem_spec = pl.BlockSpec(memory_space=pltpu.VMEM)
        dma = pltpu.SemaphoreType.DMA
        flat_rows = rows * heads
        part, factors, committed = pl.pallas_call(
            functools.partial(layer_kernel, kv, tp, proposals, heads, model_width),
            out_shape=(
                kept((kv, rows, cols), F32),
                kept((kv, rows), F32),
                kept(saved_state.shape, F32),
            ),
            in_specs=[any_spec] * 18,
            out_specs=(vmem_spec,) * 3,
            scratch_shapes=[
                pltpu.VMEM(tokens.shape, BF16),
                pltpu.VMEM((kv, rows, chunk), BF16),
                pltpu.VMEM((4, kv, chunk, width), BF16),
                pltpu.VMEM((heads, seqs, size, size), BF16),
                pltpu.VMEM((tp, width, cols), BF16),
                pltpu.VMEM((4, rows, width), F32),
                pltpu.VMEM((rows, 2 * heads * tp), F32),
                pltpu.VMEM((heads, rows, size), BF16),
                pltpu.VMEM((2, kv, heads, rows, size), BF16),
                pltpu.VMEM((kv, tp, rows, cols), BF16),
                pltpu.VMEM((kv, tp, rows, cols), BF16),
                pltpu.VMEM((kv, rows), F32),
                pltpu.VMEM((kv * tp, kv, rows), F32),
                pltpu.VMEM((1, model_width), F32),
                pltpu.VMEM((heads * tp, model_width), BF16),
                pltpu.VMEM((heads * tp, model_width), BF16),
                pltpu.VMEM((1, heads), F32),
                pltpu.VMEM((1, size), F32),
                pltpu.VMEM((1, cols), F32),
                pltpu.VMEM((flat_rows, size), BF16),
                pltpu.VMEM((flat_rows, size), BF16),
                pltpu.VMEM((proposals, heads, seqs), F32),
                pltpu.VMEM((proposals, heads, seqs), F32),
                pltpu.VMEM((1, seqs), jnp.int32),
                dma((4, kv)), dma((flat_rows // min(128, flat_rows),)), dma((tp,)), dma, dma((11,)),
                dma((kv,)), dma((kv,)),
                dma((kv, tp)), dma((kv, tp)), dma((2, kv, heads)), dma((2, kv, heads)),
                dma((kv, tp)), dma((kv, tp)), dma((kv * tp,)), dma((kv * tp,)),
            ],
            compiler_params=pltpu.CompilerParams(
                collective_id=0, has_side_effects=True, vmem_limit_bytes=VMEM_BYTES * 5 // 3 if cols % 128 else VMEM_BYTES
            ),
            name="layer",
        )(*[pltpu.with_memory_space_constraint(x, pltpu.HBM) for x in (
            tokens, pre_gain.reshape(1, model_width), query_weight, key_weight, value_weight,
            gate_weight, beta_weight.T, decay_weight.T, decay_log.reshape(1, heads), head_gain.reshape(1, size), out_w,
            post_gain.reshape(1, cols), saved_state, earlier_keys.reshape(flat_rows, size),
            earlier_values.reshape(flat_rows, size), jnp.transpose(earlier_rates, (1, 2, 0)),
            jnp.transpose(earlier_decays, (1, 2, 0)), accepted.reshape(1, seqs),
        )])
        pieces = math.gcd(seqs, 8)
        mixed_shape = (tokens.shape[0], cols)
        if cols % 128:
            mixed = pl.pallas_call(
                scale_rows, out_shape=jax.ShapeDtypeStruct(mixed_shape, BF16), name="scale"
            )(part, factors)
            return (mixed, committed)
        return pl.pallas_call(
            functools.partial(store_kernel, pieces),
            out_shape=(
                jax.ShapeDtypeStruct(mixed_shape, BF16),
                jax.ShapeDtypeStruct(committed.shape, F32),
            ),
            in_specs=[vmem_spec] * 3,
            out_specs=(any_spec, any_spec),
            scratch_shapes=[pltpu.VMEM(mixed_shape, BF16), dma((pieces + 1,))],
            compiler_params=pltpu.CompilerParams(vmem_limit_bytes=VMEM_BYTES // 4),
            name="store",
        )(*[pltpu.with_memory_space_constraint(x, pltpu.VMEM) for x in (part, factors, committed)])

    return local


def solution(mesh):
    placed = (
        P("dp", "kv"),
        P(),
        P(None, "tp"),
        P(None, "tp"),
        P(None, "tp"),
        P(None, "tp"),
        P(),
        P(),
        P("tp"),
        P(),
        P("tp", "kv"),
        P(("kv", "tp")),
        P(("dp", "kv"), "tp", None, None),
        P(("dp", "kv"), None, "tp", None),
        P(("dp", "kv"), None, "tp", None),
        P(("dp", "kv"), None, "tp"),
        P(("dp", "kv"), None, "tp"),
        P(("dp", "kv")),
    )
    return jax.shard_map(
        make_local(mesh),
        mesh=mesh,
        in_specs=placed,
        out_specs=(P("dp", ("kv", "tp")), P(("dp", "kv"), "tp", None, None)),
        check_vma=False,
    )
```

```python
import functools
import math

import jax
import jax.numpy as jnp
from jax import lax
from jax.experimental import pallas as pl
from jax.experimental.pallas import tpu as pltpu
from jax.sharding import PartitionSpec as P

F32 = jnp.float32
BF16 = jnp.bfloat16
EPS = 1e-06
MESH_IDS = pl.DeviceIdType.MESH
VMEM_BYTES = 36 * 1024 * 1024


def mm(a, b):
    return jnp.dot(a, b, preferred_element_type=F32)


def mm_nt(a, b):
    return lax.dot_general(a, b, (((1,), (1,)), ((), ())), preferred_element_type=F32)


def mm_tn(a, b):
    return lax.dot_general(a, b, (((0,), (0,)), ((), ())), preferred_element_type=F32)


def mm_exact(a, b):
    return jnp.dot(a, b, preferred_element_type=F32, precision=lax.Precision.HIGHEST)


def unit(values):
    return values * lax.rsqrt(jnp.sum(values * values, axis=-1, keepdims=True) + EPS)


def silu(values):
    return values / (1.0 + jnp.exp(-values))


def masks_of(rows, proposals):
    r = lax.broadcasted_iota(jnp.int32, (rows, rows), 0)
    c = lax.broadcasted_iota(jnp.int32, (rows, rows), 1)
    same = (r // proposals) == (c // proposals)
    return same, same & (c <= r), same & (c < r)


def per_sequence(operands, state_of, proposals, rows):
    size = operands[0].shape[1]
    group = 16
    seqs = group // proposals
    stack = group * len(operands)
    row = lax.broadcasted_iota(jnp.int32, (stack, size), 0)
    owner = (row % group) // proposals
    outs = [[] for _ in operands]
    for g in range(rows // group):
        x = jnp.concatenate([o[g * group:(g + 1) * group] for o in operands], axis=0)
        lhs = jnp.concatenate(
            [jnp.where(owner == s, x, 0.0).astype(BF16) for s in range(seqs)], axis=1
        )
        rhs = state_of(g * seqs, seqs).reshape(seqs * size, size).astype(BF16)
        y = mm(lhs, rhs)
        for i in range(len(operands)):
            outs[i].append(y[i * group:(i + 1) * group])
    return [jnp.concatenate(o, axis=0) for o in outs]


def solve(keys, values, recalled, rate, decay_pairs, gamma, strict):
    kb = keys.astype(BF16)
    low = (jnp.where(strict, decay_pairs * mm_nt(kb, kb), 0.0) * rate).astype(BF16)
    rhs = rate * (values - gamma * recalled)
    square = mm(low, low).astype(BF16)
    x = rhs + mm(square, rhs.astype(BF16))
    return x - mm(low, x.astype(BF16))


def head_masks(rows, group, heads):
    r = lax.broadcasted_iota(jnp.int32, (rows, rows), 0)
    c = lax.broadcasted_iota(jnp.int32, (rows, rows), 1)
    same = ((r // group) == (c // group)) & ((r % heads) == (c % heads))
    return same & (c <= r), same & (c < r)


def commit_table(proposals, heads, rates, decays, accepted):
    seqs = accepted.shape[1]
    live = [accepted > p for p in range(proposals)]
    rate = jnp.concatenate([jnp.where(live[p], rates[p], 0.0) for p in range(proposals)], axis=0)
    sums = [jnp.where(live[0], decays[0], 0.0)]
    for p in range(1, proposals):
        sums.append(sums[-1] + jnp.where(live[p], decays[p], 0.0))
    cum = jnp.concatenate(sums, axis=0)
    last = jnp.concatenate([sums[-1]] * proposals, axis=0)
    used = 3 * proposals * heads
    table = jnp.concatenate([rate, cum, last], axis=0)
    table = jnp.concatenate([table, jnp.zeros((used, 128 - seqs), F32)], axis=1)
    table = jnp.concatenate([table, jnp.zeros((128 - used, 128), F32)], axis=0)
    return table.T


def commit_block(block, proposals, heads, table, keys_raw, values, masks, com, sbf):
    rows, size = keys_raw.shape
    group = proposals * heads
    seqs = rows // group
    incl, strict = masks
    spread = jnp.concatenate(
        [
            jnp.broadcast_to(table[block * seqs + i:block * seqs + i + 1, :], (group, 128))
            for i in range(seqs)
        ],
        axis=0,
    )
    lane = lax.broadcasted_iota(jnp.int32, (rows, 128), 1)
    slot = lax.broadcasted_iota(jnp.int32, (rows, 128), 0) % group

    def column(k):
        return jnp.sum(jnp.where(lane == k * group + slot, spread, 0.0), axis=1, keepdims=True)

    rate, g_col, g_last = column(0), column(1), column(2)
    g_row = jnp.broadcast_to(g_col, (rows, rows)).T
    pairs = jnp.exp(jnp.where(incl, g_col - g_row, -1e30))
    keys = unit(keys_raw.astype(F32))
    owner = lax.broadcasted_iota(jnp.int32, (group, size), 0) % heads

    def widen(x):
        return jnp.concatenate(
            [jnp.where(owner == h, x, 0.0).astype(BF16) for h in range(heads)], axis=1
        )

    recalled = jnp.concatenate(
        [
            mm(
                widen(keys[i * group:(i + 1) * group]),
                com[block * seqs + i].reshape(heads * size, size).astype(BF16),
            )
            for i in range(seqs)
        ],
        axis=0,
    )
    w = solve(keys, values.astype(F32), recalled, rate, pairs, jnp.exp(g_col), strict)
    scaled_keys = (keys * jnp.exp(g_last - g_col)).astype(BF16)
    whole = jnp.broadcast_to(jnp.exp(g_last), (rows, size))
    for i in range(seqs):
        seq = block * seqs + i
        span = slice(i * group, (i + 1) * group)
        add = mm_tn(scaled_keys[span], widen(w[span]))
        for h in range(heads):
            keep = whole[i * group + h:i * group + h + 1]
            new = keep * com[seq, h] + add[:, h * size:(h + 1) * size]
            com[seq, h] = new
            sbf[h, seq] = new.astype(BF16)


def layer_kernel(
    kv, tp, proposals, heads, model_width,
    tokens, gains_h, qw, kw, vw, gw, beta_h, decay_h, log_h, head_gain_h, ow, post_h, state,
    ekeys_h, evalues_h, erates_h, edecays_h, accepted_h,
    part, factors, com,
    tokv, tok, wv, sbf, owv, acc, sacc, att, passed, give, take, sums, sumall,
    gains, beta_t, decay_t, log_rate, head_gain, post, ekeys, evalues, erates, edecays, accepted,
    w_sem, s_sem, ow_sem, own_sem, small_sem, tok_send, tok_recv, half_send, half_recv,
    att_send, att_recv, tp_send, tp_recv, sum_send, sum_recv,
):
    me = lax.axis_index("kv")
    core = lax.axis_index("tp")
    rows, chunk = tok.shape[1], tok.shape[2]
    size = head_gain.shape[1]
    cols = part.shape[2]
    weights = (qw, kw, vw, gw)

    more_left = lax.div(2 * me, kv)
    both = more_left * (kv - 1 - me) + (1 - more_left) * me

    def nearest(j):
        paired = lax.div(2 * both - j + kv, kv)
        turned = me + (1 - 2 * (j % 2)) * ((j + 1) // 2)
        beyond = me + (1 - 2 * more_left) * (j - both)
        return paired * turned + (1 - paired) * beyond

    barrier = pltpu.get_barrier_semaphore()
    group = kv * tp
    flat = me * tp + core

    def peer(o):
        other = lax.rem(flat + o, group)
        return {"kv": other // tp, "tp": lax.rem(other, tp)}

    for o in range(1, group):
        pl.semaphore_signal(barrier, inc=1, device_id=peer(o), device_id_type=MESH_IDS)

    local = {}
    local["tok"] = pltpu.make_async_copy(tokens, tokv, own_sem)
    local["tok"].start()
    pairs_small = (
        (ekeys_h, ekeys), (evalues_h, evalues), (erates_h, erates), (edecays_h, edecays),
        (accepted_h, accepted), (gains_h, gains), (beta_h, beta_t), (decay_h, decay_t),
        (log_h, log_rate), (head_gain_h, head_gain), (post_h, post),
    )
    for i, (src, dst) in enumerate(pairs_small):
        local["small", i] = pltpu.make_async_copy(src, dst, small_sem.at[i])
        local["small", i].start()
    local["tok"].wait()
    block_rows = min(128, ekeys.shape[0])
    blocks_n = ekeys.shape[0] // block_rows
    block_seqs = state.shape[0] // blocks_n
    for b in range(blocks_n):
        span = pl.ds(b * block_seqs, block_seqs)
        local["s", b] = pltpu.make_async_copy(state.at[span], com.at[span], s_sem.at[b])
        local["s", b].start()

    def fetch_weights(d):
        c = nearest(d)
        for i in range(4):
            local["w", i, d] = pltpu.make_async_copy(
                weights[i].at[pl.ds(c * chunk, chunk), :], wv.at[i, d], w_sem.at[i, d]
            )
            local["w", i, d].start()

    for o in range(tp):
        half = lax.rem(core + o, tp)
        if len(ow.shape) == 3:
            src = ow.at[half]
        else:
            src = ow.at[:, pl.ds(pl.multiple_of(half * cols, 128), cols)]
        local["o", o] = pltpu.make_async_copy(src, owv.at[o], ow_sem.at[o])
        local["o", o].start()

    pl.semaphore_wait(barrier, group - 1)

    part_rows = rows // tp
    mine_rows = pl.ds(pl.multiple_of(core * part_rows, part_rows), part_rows)
    sent = {}
    halves = {}
    for d in range(1, kv):
        c = nearest(d)
        sent[d] = pltpu.make_async_remote_copy(
            src_ref=tokv.at[
                pl.ds(pl.multiple_of(c * rows + core * part_rows, part_rows), part_rows), :
            ],
            dst_ref=tok.at[me, mine_rows],
            send_sem=tok_send.at[c],
            recv_sem=tok_recv.at[me],
            device_id={"kv": c},
            device_id_type=MESH_IDS,
        )
        sent[d].start()

    def arrival(d):
        c = nearest(d)
        return pltpu.make_async_remote_copy(
            src_ref=tok.at[c, mine_rows],
            dst_ref=tok.at[c, mine_rows],
            send_sem=tok_send.at[c],
            recv_sem=tok_recv.at[c],
            device_id={"kv": c},
            device_id_type=MESH_IDS,
        )

    def hand_over(d):
        c = nearest(d)
        arrival(d).wait_recv()
        for o in range(1, tp):
            halves[d, o] = pltpu.make_async_remote_copy(
                src_ref=tok.at[c, mine_rows],
                dst_ref=tok.at[c, mine_rows],
                send_sem=half_send.at[d, o],
                recv_sem=half_recv.at[d, o],
                device_id={"tp": lax.rem(core + o, tp)},
                device_id_type=MESH_IDS,
            )
            halves[d, o].start()

    def project(d, squares):
        if d > 0:
            for o in range(1, tp):
                halves[d, o].wait_recv()
        c = nearest(d)
        span = pl.ds(pl.multiple_of(c * chunk, 128), chunk)
        if d == 0:
            wide = tokv[pl.ds(pl.multiple_of(me * rows, rows), rows), :].astype(F32)
        else:
            wide = tok[c].astype(F32)
        scaled = (wide * gains[:, span]).astype(BF16)
        thin = mm_nt(scaled, jnp.concatenate([beta_t[:, span], decay_t[:, span]], axis=0))
        if d == 0:
            sacc[...] = thin
        else:
            sacc[...] += thin
        for i in range(4):
            local["w", i, d].wait()
            y = mm(scaled, wv[i, d])
            if d == 0:
                acc[i] = y
            else:
                acc[i] += y
        return squares + jnp.sum(wide * wide, axis=1, keepdims=True)

    for i in range(len(pairs_small)):
        local["small", i].wait()
    table = commit_table(proposals, heads, erates[...], edecays[...], accepted[...])
    commit_masks = head_masks(block_rows, proposals * heads, heads)
    squares = jnp.zeros((rows, 1), F32)
    for b in range(blocks_n):
        span = slice(b * block_rows, (b + 1) * block_rows)
        local["s", b].wait()
        for d in range(b * kv // blocks_n, (b + 1) * kv // blocks_n):
            fetch_weights(d)
        commit_block(
            b, proposals, heads, table, ekeys[span], evalues[span], commit_masks, com, sbf
        )
    for d in range(1, min(2, kv)):
        hand_over(d)
    squares = project(0, squares)
    for d in range(2, kv):
        hand_over(d)
    for d in range(1, kv):
        squares = project(d, squares)
    inverse = lax.rsqrt(squares / model_width + EPS)

    same, incl, strict = masks_of(rows, proposals)
    all_heads = heads * tp
    pad = jnp.zeros((rows, 128 - 2 * all_heads), F32)
    raw = jnp.concatenate([sacc[...] * inverse, pad], axis=1)
    raw = pltpu.roll(raw, lax.rem(128 - core * heads, 128), axis=1)
    rates = 1.0 / (1.0 + jnp.exp(-raw))
    soft = jnp.maximum(raw, 0.0) + jnp.log1p(jnp.exp(-jnp.abs(raw)))
    speed = jnp.concatenate(
        [
            jnp.zeros((1, all_heads), F32), jnp.exp(log_rate[...]),
            jnp.zeros((1, 128 - all_heads - heads), F32),
        ],
        axis=1,
    )
    cum = -speed * soft
    place = lax.broadcasted_iota(jnp.int32, (rows, 128), 0) % proposals
    step = 1
    while step < proposals:
        cum = cum + jnp.where(place >= step, pltpu.roll(cum, step, axis=0), 0.0)
        step *= 2
    cum_t = cum.T

    stride = 2

    def parent(s):
        return (s - 1) // stride * stride

    def hop(way, s, h):
        step = s - parent(s)
        if way:
            step = kv - step
        return pltpu.make_async_remote_copy(
            src_ref=att.at[h] if parent(s) == 0 else passed.at[way, parent(s), h],
            dst_ref=passed.at[way, s, h],
            send_sem=att_send.at[way, s, h],
            recv_sem=att_recv.at[way, s, h],
            device_id={"kv": lax.rem(me + step, kv)},
            device_id_type=MESH_IDS,
        )

    def arrives(way, s):
        return me - s >= 0 if way == 0 else me + s < kv

    def leaves(way, reach):
        return me + reach < kv if way == 0 else me >= reach

    def children(s):
        return [t for t in range(s + stride, s, -1) if t < kv]

    lag = 3

    def relays(s):
        return s % stride == 0 and bool(children(s))

    def at_end(way, reach):
        return me + reach == kv - 1 if way == 0 else me == reach

    def advance(turn):
        for s in range(0, kv, stride):
            h = turn - lag * (s // stride)
            if not 0 <= h < heads or not relays(s):
                continue
            for way in range(2):
                if s > 0:
                    @pl.when(arrives(way, s) & leaves(way, 1))
                    def _():
                        hop(way, s, h).wait_recv()
                for t in children(s):
                    goes = arrives(way, s) & leaves(way, t - s)
                    if t == 1:
                        goes = goes & at_end(way, 1)

                    @pl.when(goes)
                    def _():
                        hop(way, t, h).start()
        if turn == heads:
            for way in range(2):
                @pl.when(leaves(way, 1) & jnp.logical_not(at_end(way, 1)))
                def _():
                    for h in range(heads):
                        hop(way, 1, h).start()

    def gather(way, s):
        if way is None:
            return
        here = arrives(way, s)
        if relays(s):
            here = here & jnp.logical_not(leaves(way, 1))

        @pl.when(here)
        def _():
            for h in range(heads):
                hop(way, s, h).wait_recv()

    def settle():
        for s in range(0, kv, stride):
            for t in children(s):
                for way in range(2):
                    @pl.when(arrives(way, s) & leaves(way, t - s))
                    def _():
                        for h in range(heads):
                            hop(way, t, h).wait_send()

    for first in range(heads):
        batch = range(first, first + 1)
        query, key, pairs, gamma, w, asked, reads = {}, {}, {}, {}, {}, {}, {}
        recalled = {}
        for h in batch:
            block = slice(h * size, (h + 1) * size)
            query[h] = unit(silu(acc[0, :, block] * inverse)) * size ** (-0.5)
            key[h] = unit(silu(acc[1, :, block] * inverse))
            pairs[h] = jnp.exp(jnp.where(incl, cum[:, all_heads + h:all_heads + h + 1] - cum_t[all_heads + h:all_heads + h + 1, :], -1e30))
            gamma[h] = jnp.exp(cum[:, all_heads + h:all_heads + h + 1])
        for h in batch:
            recalled[h], asked[h] = per_sequence(
                [key[h], query[h]], lambda s, n, h=h: sbf[h, s:s + n], proposals, rows
            )
        for h in batch:
            value = silu(acc[2, :, h * size:(h + 1) * size] * inverse)
            w[h] = solve(key[h], value, recalled[h], rates[:, h:h + 1], pairs[h], gamma[h], strict)
        for h in batch:
            mix = (pairs[h] * mm_nt(query[h].astype(BF16), key[h].astype(BF16))).astype(BF16)
            reads[h] = gamma[h] * asked[h] + mm(mix, w[h].astype(BF16))
        for h in batch:
            gate = silu(acc[3, :, h * size:(h + 1) * size] * inverse)
            scale = lax.rsqrt(jnp.mean(reads[h] * reads[h], axis=-1, keepdims=True) + EPS)
            att[h] = (reads[h] * scale * head_gain[...] * gate).astype(BF16)
        for h in batch:
            advance(h)

    for o in range(tp):
        local["o", o].wait()

    def swap(c, o):
        return pltpu.make_async_remote_copy(
            src_ref=give.at[c, o],
            dst_ref=take.at[c, o],
            send_sem=tp_send.at[c, o],
            recv_sem=tp_recv.at[c, o],
            device_id={"tp": lax.rem(core + o, tp)},
            device_id_type=MESH_IDS,
        )

    def combine(c, pieces):
        rows_in = jnp.concatenate(pieces, axis=1)
        for o in range(1, tp):
            give[c, o] = mm(rows_in, owv[o]).astype(BF16)
            swap(c, o).start()
        part[c] = mm(rows_in, owv[0])

    def finish(c):
        own = part[c]
        for o in range(1, tp):
            swap(c, o).wait_recv()
            own = own + take[c, o].astype(F32)
        part[c] = own * post[...]
        total = jnp.sum(own * own, axis=1, keepdims=True)
        sums[pl.ds(c, 1), :] = jnp.broadcast_to(total, (rows, rows)).T[0:1]

    def blocks(s):
        if s == 0:
            return [(True, me, None)]
        return [(arrives(way, s), me - s if way == 0 else me + s, way) for way in range(2)]

    def finish_at(s):
        if s == 0:
            finish(me)
            return
        for here, c, way in blocks(s):
            @pl.when(here)
            def _():
                finish(c)

    deepest = max([s for s in range(kv) if relays(s)], default=0)
    for turn in range(heads, heads + lag * (deepest // stride)):
        advance(turn)
        if turn == heads:
            combine(me, [att[h] for h in range(heads)])
    if not deepest:
        combine(me, [att[h] for h in range(heads)])
    for s in range(1, kv):
        for here, c, way in blocks(s):
            gather(way, s)

            @pl.when(here)
            def _():
                combine(c, [passed[way, s, h] for h in range(heads)])
        finish_at(s - 1)
    finish_at(kv - 1)
    tells = {}
    for o in range(1, group):
        tells[o] = pltpu.make_async_remote_copy(
            src_ref=sums,
            dst_ref=sumall.at[o],
            send_sem=sum_send.at[o],
            recv_sem=sum_recv.at[o],
            device_id=peer(o),
            device_id_type=MESH_IDS,
        )
        tells[o].start()
    totals = sums[...]
    for o in range(1, group):
        tells[o].wait_recv()
        totals = totals + sumall[o]
    factors[...] = lax.rsqrt(totals / model_width + EPS)
    for o in range(1, group):
        tells[o].wait_send()
    settle()
    for d in range(1, kv):
        sent[d].wait_send()
        for o in range(1, tp):
            halves[d, o].wait_send()
    for c in range(kv):
        for o in range(1, tp):
            swap(c, o).wait_send()


def scale_rows(part, factors, mixed):
    kv, rows, cols = part.shape
    for c in range(kv):
        factor = jnp.broadcast_to(factors[c:c + 1, :], (rows, rows)).T[:, 0:1]
        mixed[c * rows:(c + 1) * rows, :] = (part[c] * factor).astype(BF16)


def store_kernel(pieces, part, factors, com, mixed_out, com_out, mixed, sems):
    copies = []
    size = com.shape[0] // pieces
    for i in range(pieces):
        span = pl.ds(i * size, size)
        copies.append(pltpu.make_async_copy(com.at[span], com_out.at[span], sems.at[i]))
    for copy in copies:
        copy.start()
    scale_rows(part, factors, mixed)
    copies.append(pltpu.make_async_copy(mixed, mixed_out, sems.at[pieces]))
    copies[-1].start()
    for copy in copies:
        copy.wait()


def make_local(mesh):
    kv = mesh.shape["kv"]
    tp = mesh.shape["tp"]

    def local(
        tokens, pre_gain, query_weight, key_weight, value_weight, gate_weight, beta_weight,
        decay_weight, decay_log, head_gain, out_weight, post_gain, saved_state, earlier_keys,
        earlier_values, earlier_rates, earlier_decays, accepted,
    ):
        seqs, heads, size = saved_state.shape[:3]
        proposals = earlier_keys.shape[1]
        rows = seqs * proposals
        width = heads * size
        model_width = pre_gain.shape[0]
        chunk = tokens.shape[1]
        cols = post_gain.shape[0]
        if cols % 128:
            out_w = jnp.moveaxis(out_weight.reshape(width, tp, cols), 1, 0)
        else:
            out_w = out_weight
        kept = jax.ShapeDtypeStruct if cols % 128 else pltpu.VMEM
        any_spec = pl.BlockSpec(memory_space=pltpu.HBM)
        vmem_spec = pl.BlockSpec(memory_space=pltpu.VMEM)
        dma = pltpu.SemaphoreType.DMA
        flat_rows = rows * heads
        part, factors, committed = pl.pallas_call(
            functools.partial(layer_kernel, kv, tp, proposals, heads, model_width),
            out_shape=(
                kept((kv, rows, cols), F32),
                kept((kv, rows), F32),
                kept(saved_state.shape, F32),
            ),
            in_specs=[any_spec] * 18,
            out_specs=(vmem_spec,) * 3,
            scratch_shapes=[
                pltpu.VMEM(tokens.shape, BF16),
                pltpu.VMEM((kv, rows, chunk), BF16),
                pltpu.VMEM((4, kv, chunk, width), BF16),
                pltpu.VMEM((heads, seqs, size, size), BF16),
                pltpu.VMEM((tp, width, cols), BF16),
                pltpu.VMEM((4, rows, width), F32),
                pltpu.VMEM((rows, 2 * heads * tp), F32),
                pltpu.VMEM((heads, rows, size), BF16),
                pltpu.VMEM((2, kv, heads, rows, size), BF16),
                pltpu.VMEM((kv, tp, rows, cols), BF16),
                pltpu.VMEM((kv, tp, rows, cols), BF16),
                pltpu.VMEM((kv, rows), F32),
                pltpu.VMEM((kv * tp, kv, rows), F32),
                pltpu.VMEM((1, model_width), F32),
                pltpu.VMEM((heads * tp, model_width), BF16),
                pltpu.VMEM((heads * tp, model_width), BF16),
                pltpu.VMEM((1, heads), F32),
                pltpu.VMEM((1, size), F32),
                pltpu.VMEM((1, cols), F32),
                pltpu.VMEM((flat_rows, size), BF16),
                pltpu.VMEM((flat_rows, size), BF16),
                pltpu.VMEM((proposals, heads, seqs), F32),
                pltpu.VMEM((proposals, heads, seqs), F32),
                pltpu.VMEM((1, seqs), jnp.int32),
                dma((4, kv)), dma((flat_rows // min(128, flat_rows),)), dma((tp,)), dma, dma((11,)),
                dma((kv,)), dma((kv,)),
                dma((kv, tp)), dma((kv, tp)), dma((2, kv, heads)), dma((2, kv, heads)),
                dma((kv, tp)), dma((kv, tp)), dma((kv * tp,)), dma((kv * tp,)),
            ],
            compiler_params=pltpu.CompilerParams(
                collective_id=0, has_side_effects=True, vmem_limit_bytes=VMEM_BYTES * 5 // 3 if cols % 128 else VMEM_BYTES
            ),
            name="layer",
        )(*[pltpu.with_memory_space_constraint(x, pltpu.HBM) for x in (
            tokens, pre_gain.reshape(1, model_width), query_weight, key_weight, value_weight,
            gate_weight, beta_weight.T, decay_weight.T, decay_log.reshape(1, heads), head_gain.reshape(1, size), out_w,
            post_gain.reshape(1, cols), saved_state, earlier_keys.reshape(flat_rows, size),
            earlier_values.reshape(flat_rows, size), jnp.transpose(earlier_rates, (1, 2, 0)),
            jnp.transpose(earlier_decays, (1, 2, 0)), accepted.reshape(1, seqs),
        )])
        pieces = math.gcd(seqs, 8)
        mixed_shape = (tokens.shape[0], cols)
        if cols % 128:
            mixed = pl.pallas_call(
                scale_rows, out_shape=jax.ShapeDtypeStruct(mixed_shape, BF16), name="scale"
            )(part, factors)
            return (mixed, committed)
        return pl.pallas_call(
            functools.partial(store_kernel, pieces),
            out_shape=(
                jax.ShapeDtypeStruct(mixed_shape, BF16),
                jax.ShapeDtypeStruct(committed.shape, F32),
            ),
            in_specs=[vmem_spec] * 3,
            out_specs=(any_spec, any_spec),
            scratch_shapes=[pltpu.VMEM(mixed_shape, BF16), dma((pieces + 1,))],
            compiler_params=pltpu.CompilerParams(vmem_limit_bytes=VMEM_BYTES // 4),
            name="store",
        )(*[pltpu.with_memory_space_constraint(x, pltpu.VMEM) for x in (part, factors, committed)])

    return local


def solution(mesh):
    placed = (
        P("dp", "kv"),
        P(),
        P(None, "tp"),
        P(None, "tp"),
        P(None, "tp"),
        P(None, "tp"),
        P(),
        P(),
        P("tp"),
        P(),
        P("tp", "kv"),
        P(("kv", "tp")),
        P(("dp", "kv"), "tp", None, None),
        P(("dp", "kv"), None, "tp", None),
        P(("dp", "kv"), None, "tp", None),
        P(("dp", "kv"), None, "tp"),
        P(("dp", "kv"), None, "tp"),
        P(("dp", "kv")),
    )
    return jax.shard_map(
        make_local(mesh),
        mesh=mesh,
        in_specs=placed,
        out_specs=(P("dp", ("kv", "tp")), P(("dp", "kv"), "tp", None, None)),
        check_vma=False,
    )
```
